128 devices in a mesh: sp: 16 (over z, x), tp: 8 (over y, core).
Axes of the slice: x: 4, y: 4, z: 4, core: 2. Of those that a mesh axis runs over, the one named last changes fastest.
Arguments:
- tokens: bfloat16 [4096, 3072], P('sp', 'tp'), may hold values from -6 to 6
- norm_gain: float32 [3072], replicated, may hold values from 0.1 to 1.9
- state_in_weight: bfloat16 [3072, 1024], P('sp', 'tp'), may hold values from -0.109375 to 0.109375
- pool_in_weight: bfloat16 [3072, 1024], P('sp', 'tp'), may hold values from -0.109375 to 0.109375
- rate_real: float32 [64, 64], replicated, may hold values from -1.5 to -0.5
- rate_imag: float32 [64, 64], replicated, may hold values from 0 to 200
- log_step: float32 [64], replicated, may hold values from -2 to 0.7
- input_real: float32 [64, 64, 16], replicated, may hold values from -1 to 1
- input_imag: float32 [64, 64, 16], replicated, may hold values from -1 to 1
- output_real: float32 [64, 16, 64], replicated, may hold values from -112 to 112
- output_imag: float32 [64, 16, 64], replicated, may hold values from -112 to 112
- skip_gain: float32 [1024], replicated, may hold values from -3 to 3
- pool_weight: bfloat16 [16, 64, 64], replicated, may hold values from -0.75 to 0.75
- pool_gain: float32 [1024], replicated, may hold values from 0.1 to 1.9
- state_out_weight: bfloat16 [1024, 3072], P('sp', 'tp'), may hold values from -0.125 to 0.125
- pool_out_weight: bfloat16 [1024, 3072], P('sp', 'tp'), may hold values from -0.125 to 0.125
Outputs:
- mixer_output: bfloat16 [4096, 3072], P('sp', 'tp')
The draws below stay inside these ranges and needn't reach their ends.
All inputs are finite; a program needn't handle non-finite values.
Results may differ from the reference program's by a relative error of at most 0.0065.
Values may be sent and summed in bfloat16 or wider, within the bound.
No kernel may reach another device: no remote copies, remote signals or barrier semaphores. Data moves between devices by JAX's collectives and lax.ppermute only.
A program may use at most 64 MiB of HBM per device.

```python
import jax
import jax.numpy as jnp
from jax import lax

D = 3072
SSM_GROUP = 16
SSM_GROUPS = 64
SSM_STATE = 64
POOL_GROUP = 64
POOL_GROUPS = 16
TOKENS = 4096
D_SSM = 1024
D_POOL = 1024


def level_of(key, dims, cuts, smallest, largest):
    gain, own = 1.0, jax.random.fold_in(key, 6)
    for axis_at, shards_of in cuts:
        draws = jnp.exp(jax.random.uniform(jax.random.fold_in(own, axis_at), (shards_of,), jnp.float32, smallest / len(cuts), largest / len(cuts)))
        gain = gain * jnp.repeat(draws, dims[axis_at] // shards_of).reshape([-1 if axis == axis_at else 1 for axis in range(len(dims))])
    return gain


def normal_values(rng, extent, scale, limit, split=(), held_as=jnp.bfloat16):
    array = scale * jax.random.normal(rng, extent, jnp.float32)
    if split:
        array = array * level_of(rng, extent, split, -0.22, 0.18)
    return jnp.clip(array, -limit, limit).astype(held_as)


def setup_inputs(seed: int = 0) -> dict:
    streams_of = jax.random.split(jax.random.key(seed), 17)
    return {
        "tokens": normal_values(streams_of[0], (TOKENS, D), 1.0, 6.0, ((0, 16), (1, 8))),
        "norm_gain": jnp.clip(1.0 + 0.18 * jax.random.normal(streams_of[1], (D,), jnp.float32), 0.1, 1.9),
        "state_in_weight": normal_values(streams_of[2], (D, D_SSM), D ** -0.5, 0.109375, ((0, 16), (1, 8))),
        "pool_in_weight": normal_values(streams_of[3], (D, D_POOL), D ** -0.5, 0.109375, ((0, 16), (1, 8))),
        "rate_real": jnp.clip(jax.random.uniform(streams_of[4], (SSM_GROUPS, SSM_STATE), jnp.float32, -1.5, -0.5), -1.5, -0.5),
        "rate_imag": jnp.clip(jax.random.uniform(streams_of[5], (SSM_GROUPS, SSM_STATE), jnp.float32, 0.0, 200.0), 0.0, 200.0),
        "log_step": jnp.clip(jax.random.uniform(streams_of[6], (SSM_GROUPS,), jnp.float32, -2.0, 0.7), -2.0, 0.7),
        "input_real": normal_values(streams_of[7], (SSM_GROUPS, SSM_STATE, SSM_GROUP), (2 * SSM_GROUP) ** -0.5, 1.0, (), jnp.float32),
        "input_imag": normal_values(streams_of[8], (SSM_GROUPS, SSM_STATE, SSM_GROUP), (2 * SSM_GROUP) ** -0.5, 1.0, (), jnp.float32),
        "output_real": normal_values(streams_of[9], (SSM_GROUPS, SSM_GROUP, SSM_STATE), (TOKENS // 256 + 2), 112.0, (), jnp.float32),
        "output_imag": normal_values(streams_of[10], (SSM_GROUPS, SSM_GROUP, SSM_STATE), (TOKENS // 256 + 2), 112.0, (), jnp.float32),
        "skip_gain": normal_values(streams_of[11], (D_SSM,), 0.5, 3.0, (), jnp.float32),
        "pool_weight": normal_values(streams_of[12], (POOL_GROUPS, POOL_GROUP, POOL_GROUP), POOL_GROUP ** -0.5, 0.75),
        "pool_gain": jnp.clip(1.0 + 0.18 * jax.random.normal(streams_of[13], (D_POOL,), jnp.float32), 0.1, 1.9),
        "state_out_weight": normal_values(streams_of[14], (D_SSM, D), (D_SSM + D_POOL) ** -0.5, 0.125, ((0, 16), (1, 8))),
        "pool_out_weight": normal_values(streams_of[15], (D_POOL, D), (D_SSM + D_POOL) ** -0.5, 0.125, ((0, 16), (1, 8))),
    }


epsilon = 1e-06
highest = lax.Precision.HIGHEST

def discretize(rate_real, rate_imag, log_step, length):
    step_size = jnp.exp(log_step)[:, None] / length
    exponent = rate_real * step_size
    angle = rate_imag * step_size
    magnitude = jnp.exp(exponent)
    decay_real = magnitude * jnp.cos(angle)
    decay_imag = magnitude * jnp.sin(angle)
    less_one = jnp.expm1(exponent) * jnp.cos(angle) - 2.0 * jnp.square(jnp.sin(0.5 * angle))
    denominator = rate_real * rate_real + rate_imag * rate_imag
    factor_real = (less_one * rate_real + decay_imag * rate_imag) / denominator
    factor_imag = (decay_imag * rate_real - less_one * rate_imag) / denominator
    return (exponent, angle, decay_real, decay_imag, factor_real, factor_imag)

def drive_terms(signal, factor_real, factor_imag, input_real, input_imag):
    drive_real = factor_real[..., None] * input_real - factor_imag[..., None] * input_imag
    drive_imag = factor_real[..., None] * input_imag + factor_imag[..., None] * input_real
    push_real = jnp.einsum('tgc,gnc->tgn', signal, drive_real, precision=highest)
    push_imag = jnp.einsum('tgc,gnc->tgn', signal, drive_imag, precision=highest)
    return (push_real, push_imag)

def readout(states_real, states_imag, output_real, output_imag, signal, skip_gain):
    row_count = states_real.shape[0]
    readout_sum = jnp.einsum('tgn,gcn->tgc', states_real, output_real, precision=highest)
    readout_sum = readout_sum - jnp.einsum('tgn,gcn->tgc', states_imag, output_imag, precision=highest)
    readout_sum = readout_sum.reshape(row_count, -1) + skip_gain * signal.reshape(row_count, -1)
    return jax.nn.gelu(readout_sum).astype(jnp.bfloat16)

def pool_mixer(pool_in, pool_weight, pool_gain):
    row_count = pool_in.shape[0]
    signal = pool_in.astype(jnp.float32).reshape(row_count, POOL_GROUPS, POOL_GROUP)
    running = jnp.cumsum(signal, axis=0)
    padded = jnp.pad(running, ((16, 0), (0, 0), (0, 0)))
    positions = jnp.arange(1, row_count + 1)
    window_means = []
    for group_index in range(POOL_GROUPS):
        window = 2 ** (group_index % 4 + 1)
        lagged = padded[16 - window:16 - window + row_count, group_index]
        divisor = jnp.minimum(positions, window).astype(jnp.float32)[:, None]
        window_means.append((running[:, group_index] - lagged) / divisor)
    pooled = jnp.stack(window_means, axis=1) - signal
    projected = jnp.einsum('tgc,gcd->tgd', pooled, pool_weight.astype(jnp.float32), precision=highest)
    return (projected.reshape(row_count, -1) * pool_gain).astype(jnp.bfloat16)

def reference(tokens, norm_gain, state_in_weight, pool_in_weight, rate_real, rate_imag, log_step, input_real, input_imag, output_real, output_imag, skip_gain, pool_weight, pool_gain, state_out_weight, pool_out_weight):
    features = tokens.astype(jnp.float32)
    inverse = lax.rsqrt(lax.optimization_barrier(jnp.sum(features * features, axis=1)) / D + epsilon)[:, None]
    scaled = (features * norm_gain).astype(jnp.bfloat16)
    state_in = (jnp.dot(scaled, state_in_weight, preferred_element_type=jnp.float32) * inverse).astype(jnp.bfloat16)
    pool_in = (jnp.dot(scaled, pool_in_weight, preferred_element_type=jnp.float32) * inverse).astype(jnp.bfloat16)
    signal = state_in.astype(jnp.float32).reshape(TOKENS, SSM_GROUPS, SSM_GROUP)
    exponent, angle, decay_real, decay_imag, factor_real, factor_imag = discretize(rate_real, rate_imag, log_step, TOKENS)
    push_real, push_imag = drive_terms(signal, factor_real, factor_imag, input_real, input_imag)

    def advance(carry, pushes):
        state_real, state_imag = carry
        next_real = decay_real * state_real - decay_imag * state_imag + pushes[0]
        next_imag = decay_real * state_imag + decay_imag * state_real + pushes[1]
        return ((next_real, next_imag), (next_real, next_imag))
    zero_state = jnp.zeros((SSM_GROUPS, SSM_STATE), jnp.float32)
    _, (states_real, states_imag) = lax.scan(advance, (zero_state, zero_state), (push_real, push_imag))
    state_out = readout(states_real, states_imag, output_real, output_imag, signal, skip_gain)
    pool_out = pool_mixer(pool_in, pool_weight, pool_gain)
    combined = jnp.dot(state_out, state_out_weight, preferred_element_type=jnp.float32)
    combined = combined + jnp.dot(pool_out, pool_out_weight, preferred_element_type=jnp.float32)
    return combined.astype(jnp.bfloat16)
```

```python
import functools

import jax
import jax.numpy as jnp
from jax import lax
from jax.experimental import pallas as pl
from jax.experimental.pallas import tpu as pltpu
from jax.sharding import Mesh
from jax.sharding import PartitionSpec as P

SP = ("z", "x")
TP = ("y", "c")
RING = 4
ROWS = 256
WIDTH = 3072
SLICE = 384
LENGTH = 4096
CH = 128
GROUPS = 8
COLS = 512
HALO = 16
epsilon = 1e-06

bf16, f32 = jnp.bfloat16, jnp.float32


def call(body, outs, *args, scratch=(), in_specs=None):
    shapes = [jax.ShapeDtypeStruct(shape, dtype) for shape, dtype in outs]
    single = len(shapes) == 1
    vmem = pl.BlockSpec(memory_space=pltpu.VMEM)
    return pl.pallas_call(
        body,
        out_shape=shapes[0] if single else shapes,
        in_specs=in_specs if in_specs is not None else [vmem] * len(args),
        out_specs=vmem if single else [vmem] * len(shapes),
        scratch_shapes=list(scratch),
    )(*args)


def iota(shape, dim):
    return lax.broadcasted_iota(jnp.int32, shape, dim)


def where_am_i():
    z, x, y, c = (lax.axis_index(a) for a in ("z", "x", "y", "c"))
    return z, x, y, c


def ring(index, back):
    return lax.rem(index + RING - back, RING)


def nt(a, b):
    return lax.dot_general(a, b, (((1,), (1,)), ((), ())), preferred_element_type=f32)


def split(value):
    high = value.astype(bf16)
    return high, (value - high.astype(f32)).astype(bf16)


def pack_kernel(ws, wp, os, op, m):
    m[0:192] = ws[...]
    m[192:384] = wp[...]
    for j in range(3):
        m[384 + 64 * j : 448 + 64 * j] = os[:, 128 * j : 128 * (j + 1)]
        m[576 + 64 * j : 640 + 64 * j] = op[:, 128 * j : 128 * (j + 1)]


def rows_in_kernel(m0, m1, m2, m3, zs):
    x = lax.axis_index("x")
    for k, m in enumerate((m0, m1, m2, m3)):
        at = pl.multiple_of(ring(x, k) * 192, 64)
        zs[pl.ds(at, 192)] = m[0:192]


def rows_rest_kernel(m0, m1, m2, m3, zp, zo):
    x = lax.axis_index("x")
    for k, m in enumerate((m0, m1, m2, m3)):
        from_x = ring(x, k)
        at = pl.multiple_of(from_x * 192, 64)
        zp[pl.ds(at, 192)] = m[192:384]
        at = pl.multiple_of(from_x * 64, 64)
        for b in range(2):
            for j in range(3):
                first = 384 + 192 * b + 64 * j
                zo[b, pl.ds(at, 64), 128 * j : 128 * (j + 1)] = m[first : first + 64]


def power(exponent, angle, count):
    size = jnp.exp(exponent * count)
    return size * jnp.cos(angle * count), size * jnp.sin(angle * count)


def tables_kernel(
    rr, ri, ls, inr, ini, outr, outi, pw, d_ref, r_ref, t_ref, b_ref,
    rr_v, ri_v, inr_v, ini_v, outr_v, outi_v, pw_v, sems,
):
    z, x, y, c = where_am_i()
    t = y * 2 + c
    s = z * RING + x
    g0 = pl.multiple_of(t * GROUPS, GROUPS)
    moves = [
        (rr.at[pl.ds(g0, GROUPS)], rr_v),
        (ri.at[pl.ds(g0, GROUPS)], ri_v),
        (inr.at[pl.ds(g0, GROUPS)], inr_v),
        (ini.at[pl.ds(g0, GROUPS)], ini_v),
        (outr.at[pl.ds(g0, GROUPS)], outr_v),
        (outi.at[pl.ds(g0, GROUPS)], outi_v),
        (pw.at[pl.ds(t * 2, 2)], pw_v),
    ]
    copies = [pltpu.make_async_copy(src, dst, sems.at[k]) for k, (src, dst) in enumerate(moves)]
    for copy in copies:
        copy.start()
    for copy in copies:
        copy.wait()

    spread = (iota((64, COLS), 0) == iota((64, COLS), 1) % 64).astype(f32)
    own_row = iota((GROUPS, COLS), 1) // 64 == iota((GROUPS, COLS), 0)

    def flat(value):
        wide = jnp.dot(value, spread, precision=lax.Precision.HIGHEST, preferred_element_type=f32)
        return jnp.sum(jnp.where(own_row, wide, 0.0), axis=0, keepdims=True)

    logs = jnp.broadcast_to(ls[...], (GROUPS, 64))
    mine = iota((GROUPS, 64), 1) == iota((GROUPS, 64), 0) + g0
    step = jnp.exp(jnp.sum(jnp.where(mine, logs, 0.0), axis=1, keepdims=True)) / LENGTH
    rate_r, rate_i = flat(rr_v[...]), flat(ri_v[...])
    step = flat(jnp.broadcast_to(step, (GROUPS, 64)))
    exponent, angle = rate_r * step, rate_i * step
    decay_i = jnp.exp(exponent) * jnp.sin(angle)
    grown = exponent * (1.0 + exponent * (0.5 + exponent * (1.0 / 6.0 + exponent * (1.0 / 24.0))))
    half = jnp.sin(0.5 * angle)
    less_one = grown * jnp.cos(angle) - 2.0 * half * half
    below = rate_r * rate_r + rate_i * rate_i
    factor_r = (less_one * rate_r + decay_i * rate_i) / below
    factor_i = (decay_i * rate_r - less_one * rate_i) / below

    tall = (iota((CH, 16), 0) % 16 == iota((CH, 16), 1)).astype(f32)
    same = iota((CH, COLS), 0) // 16 == iota((CH, COLS), 1) // 64

    def across(value):
        return lax.dot_general(
            tall, value[...].reshape(COLS, 16), (((1,), (1,)), ((), ())),
            precision=lax.Precision.HIGHEST, preferred_element_type=f32,
        )

    in_r, in_i = across(inr_v), across(ini_v)
    for part, value in ((0, factor_r * in_r - factor_i * in_i), (1, factor_r * in_i + factor_i * in_r)):
        high, low = split(jnp.where(same, value, 0.0))
        d_ref[0:CH, COLS * part : COLS * (part + 1)] = high
        d_ref[CH : 2 * CH, COLS * part : COLS * (part + 1)] = low

    for part, (value, sign) in enumerate(((outr_v, 1.0), (outi_v, -1.0))):
        wide = jnp.dot(
            value[...].reshape(CH, 64), spread, precision=lax.Precision.HIGHEST, preferred_element_type=f32
        )
        high, low = split(jnp.where(same, sign * wide, 0.0))
        r_ref[0:CH, COLS * part : COLS * (part + 1)] = high
        r_ref[CH : 2 * CH, COLS * part : COLS * (part + 1)] = low

    row = iota((8, COLS), 0)
    for k, shift in enumerate((1, 2, 4)):
        real, imag = power(exponent, angle, float(shift))
        t_ref[16 * k : 16 * k + 8] = jnp.where(row >= shift, real, 0.0)
        t_ref[16 * k + 8 : 16 * k + 16] = jnp.where(row >= shift, imag, 0.0)
    t_ref[48:56], t_ref[56:64] = power(exponent, angle, (row + 1).astype(f32))
    gap = s - 1 - iota((16, COLS), 0)
    real, imag = power(exponent, angle, (ROWS * jnp.maximum(gap, 0)).astype(f32))
    t_ref[64:80] = jnp.where(gap >= 0, real, 0.0)
    t_ref[80:96] = jnp.where(gap >= 0, imag, 0.0)

    pick = (iota((64, CH), 0) == iota((64, CH), 1) % 64).astype(bf16)
    wide = jnp.dot(pw_v[...].reshape(CH, 64), pick, preferred_element_type=f32)
    wide = jnp.where(iota((CH, CH), 0) // 64 == iota((CH, CH), 1) // 64, wide, 0.0).astype(bf16)
    b_ref[0:CH] = wide
    b_ref[CH : 2 * CH] = wide


def scale_kernel(*refs):
    tokens, gain, scaled, inverse = refs[:8], refs[8], refs[9], refs[10]
    _, _, y, c = where_am_i()
    total = jnp.zeros((ROWS, 128), f32)
    for k in range(8):
        from_y, from_c = ring(y, k % 4), c if k < 4 else 1 - c
        t = from_y * 2 + from_c
        for j in range(3):
            value = tokens[k][:, 128 * j : 128 * (j + 1)].astype(f32)
            total += value * value
            scaled[t, :, 128 * j : 128 * (j + 1)] = (value * gain[pl.ds(3 * t + j, 1)]).astype(bf16)
    squares = jnp.sum(total, axis=1, keepdims=True)
    inverse[...] = jnp.broadcast_to(lax.rsqrt(squares / WIDTH + epsilon), (ROWS, 128))


def project(scaled, weights, inverse):
    z = lax.axis_index("z")
    total = jnp.zeros((ROWS, CH), f32)
    for k in range(RING):
        at = ring(z, k) * 2
        left = jnp.concatenate([scaled[at], scaled[at + 1]], axis=1)
        total += jnp.dot(left, weights[k][...], preferred_element_type=f32)
    return (total * inverse[...]).astype(bf16)


def state_kernel(scaled, inverse, w0, w1, w2, w3, d, t, x_ref, end, state_in, push):
    value = project(scaled, (w0, w1, w2, w3), inverse)
    state_in[...] = value
    push[...] = jnp.dot(jnp.concatenate([value, value], axis=1), d[...], preferred_element_type=f32)
    for j in range(4):
        at_r, at_i = slice(128 * j, 128 * (j + 1)), slice(COLS + 128 * j, COLS + 128 * (j + 1))
        levels = [(1 << k, t[16 * k : 16 * k + 8, at_r], t[16 * k + 8 : 16 * k + 16, at_r]) for k in range(3)]
        by_r, by_i = t[55:56, at_r], t[63:64, at_r]
        sum_r, sum_i = jnp.zeros((8, 128), f32), jnp.zeros((8, 128), f32)
        for k in range(ROWS // 8):
            rows = slice(8 * k, 8 * k + 8)
            real, imag = push[rows, at_r], push[rows, at_i]
            for shift, mul_r, mul_i in levels:
                old_r, old_i = pltpu.roll(real, shift, 0), pltpu.roll(imag, shift, 0)
                real, imag = real + mul_r * old_r - mul_i * old_i, imag + mul_r * old_i + mul_i * old_r
            x_ref[rows, at_r] = real
            x_ref[rows, at_i] = imag
            sum_r, sum_i = sum_r * by_r - sum_i * by_i + real, sum_r * by_i + sum_i * by_r + imag
        end[j : j + 1] = sum_r[7:8]
        end[4 + j : 5 + j] = sum_i[7:8]


def pool_in_kernel(scaled, inverse, w0, w1, w2, w3, pool_in, tail):
    value = project(scaled, (w0, w1, w2, w3), inverse)
    pool_in[...] = value
    tail[...] = value[ROWS - HALO :]


def mix_kernel(x_ref, ends, t, r, state_in, skip, pool_in, halo, b, gain, outs, high, low):
    z, x, y, c = where_am_i()
    s = z * RING + x
    me = y * 2 + c
    carries = []
    for j in range(4):
        cols = slice(128 * j, 128 * (j + 1))
        real, imag = ends[:, j, :], ends[:, 4 + j, :]
        mul_r, mul_i = t[64:80, cols], t[80:96, cols]
        carries.append(
            [
                jnp.sum(mul_r * real - mul_i * imag, axis=0, keepdims=True),
                jnp.sum(mul_r * imag + mul_i * real, axis=0, keepdims=True),
            ]
        )
    for k in range(ROWS // 16):
        for j in range(4):
            at_r, at_i = slice(128 * j, 128 * (j + 1)), slice(COLS + 128 * j, COLS + 128 * (j + 1))
            base_r, base_i = t[48:56, at_r], t[56:64, at_r]
            both_r, both_i = [], []
            for h in range(2):
                rows = slice(16 * k + 8 * h, 16 * k + 8 * h + 8)
                old_r, old_i = carries[j]
                real = x_ref[rows, at_r] + (base_r * old_r - base_i * old_i)
                imag = x_ref[rows, at_i] + (base_r * old_i + base_i * old_r)
                carries[j] = [real[7:8], imag[7:8]]
                both_r.append(real)
                both_i.append(imag)
            rows = slice(16 * k, 16 * k + 16)
            for at, both in ((at_r, both_r), (at_i, both_i)):
                high[rows, at], low[rows, at] = split(jnp.concatenate(both, axis=0))
    wide = nt(high[...], r[...])
    total = wide[:, 0:CH] + (wide[:, CH : 2 * CH] + nt(low[...], r[0:CH]))
    total = total + skip[pl.ds(me, 1)] * state_in[...].astype(f32)
    outs[:, 0:CH] = jax.nn.gelu(total).astype(bf16)

    own = pool_in[...].astype(f32)
    ext = jnp.concatenate([halo[...].astype(f32), own], axis=0)
    sums = []
    for k in range(4):
        ext = ext + pltpu.roll(ext, 1 << k, 0)
        sums.append(ext[HALO:])
    lane = iota((ROWS, CH), 1)
    odd = me % 2 == 1
    near = jnp.where(odd, sums[2], sums[0])
    far = jnp.where(odd, sums[3], sums[1])
    window = jnp.where(odd, jnp.where(lane < 64, 8, 16), jnp.where(lane < 64, 2, 4))
    count = jnp.minimum(s * ROWS + 1 + iota((ROWS, CH), 0), window).astype(f32)
    pooled = jnp.where(lane < 64, near, far) / count - own
    pair = jnp.concatenate(split(pooled), axis=1)
    outs[:, CH : 2 * CH] = (
        jnp.dot(pair, b[...], preferred_element_type=f32) * gain[pl.ds(me, 1)]
    ).astype(bf16)


def final_kernel(*refs):
    outs, weights, out, held = refs[:8], refs[8:12], refs[12], refs[13]
    z, _, y, c = where_am_i()
    for k in range(8):
        from_y, from_c = ring(y, k % 4), c if k < 4 else 1 - c
        held[from_y * 2 + from_c] = outs[k][...]
    total = jnp.zeros((ROWS, SLICE), f32)
    for k in range(RING):
        at = ring(z, k) * 2
        first, second = held[at], held[at + 1]
        for b in range(2):
            cols = slice(CH * b, CH * (b + 1))
            left = jnp.concatenate([first[:, cols], second[:, cols]], axis=1)
            total += jnp.dot(left, weights[k][b], preferred_element_type=f32)
    out[...] = total.astype(bf16)


def around(value, axis):
    return [
        lax.ppermute(value, axis, [(i, (i + k) % RING) for i in range(RING)]) for k in range(1, RING)
    ]


def partner(value):
    return lax.ppermute(value, "c", [(0, 1), (1, 0)])


def body(
    tokens,
    norm_gain,
    state_in_weight,
    pool_in_weight,
    rate_real,
    rate_imag,
    log_step,
    input_real,
    input_imag,
    output_real,
    output_imag,
    skip_gain,
    pool_weight,
    pool_gain,
    state_out_weight,
    pool_out_weight,
):
    packed = call(
        pack_kernel, [((768, 128), bf16)], state_in_weight, pool_in_weight, state_out_weight, pool_out_weight
    )
    over_x = [packed, *around(packed, "x")]
    over_y = [tokens, *around(tokens, "y")]
    blocks = over_y + [partner(part) for part in over_y]

    anywhere = pl.BlockSpec(memory_space=pl.ANY)
    vmem = pl.BlockSpec(memory_space=pltpu.VMEM)
    drive, read, table, mixer = call(
        tables_kernel,
        [((2 * CH, 2 * COLS), bf16), ((2 * CH, 2 * COLS), bf16), ((96, COLS), f32), ((2 * CH, CH), bf16)],
        rate_real, rate_imag, log_step.reshape(1, 64), input_real, input_imag, output_real, output_imag, pool_weight,
        in_specs=[anywhere, anywhere, vmem, anywhere, anywhere, anywhere, anywhere, anywhere],
        scratch=[
            pltpu.VMEM((GROUPS, 64), f32),
            pltpu.VMEM((GROUPS, 64), f32),
            pltpu.VMEM((GROUPS, 64, 16), f32),
            pltpu.VMEM((GROUPS, 64, 16), f32),
            pltpu.VMEM((GROUPS, 16, 64), f32),
            pltpu.VMEM((GROUPS, 16, 64), f32),
            pltpu.VMEM((2, 64, 64), bf16),
            pltpu.SemaphoreType.DMA((7,)),
        ],
    )

    rows_s = call(rows_in_kernel, [((768, 128), bf16)], *over_x)
    rows_p, rows_o = call(rows_rest_kernel, [((768, 128), bf16), ((2, 256, SLICE), bf16)], *over_x)
    state_rows = [rows_s, *around(rows_s, "z")]
    pool_rows = [rows_p, *around(rows_p, "z")]
    out_rows = [rows_o, *around(rows_o, "z")]

    scaled, inverse = call(
        scale_kernel,
        [((8, ROWS, SLICE), bf16), ((ROWS, 128), f32)],
        *blocks,
        norm_gain.reshape(24, 128),
    )
    local, end, state_in = call(
        state_kernel,
        [((ROWS, 2 * COLS), f32), ((8, 128), f32), ((ROWS, CH), bf16)],
        scaled,
        inverse,
        *state_rows,
        drive,
        table,
        scratch=[pltpu.VMEM((ROWS, 2 * COLS), f32)],
    )
    ends = lax.all_to_all(jnp.broadcast_to(end[None], (16, 8, 128)), SP, 0, 0, tiled=True)
    pool_in, tail = call(
        pool_in_kernel, [((ROWS, CH), bf16), ((HALO, CH), bf16)], scaled, inverse, *pool_rows
    )
    halo = lax.ppermute(tail, SP, [(i, i + 1) for i in range(15)])
    outs = call(
        mix_kernel,
        [((ROWS, 2 * CH), bf16)],
        local,
        ends,
        table,
        read,
        state_in,
        skip_gain.reshape(8, 128),
        pool_in,
        halo,
        mixer,
        pool_gain.reshape(8, 128),
        scratch=[pltpu.VMEM((ROWS, 2 * COLS), bf16), pltpu.VMEM((ROWS, 2 * COLS), bf16)],
    )
    over_y = [outs, *around(outs, "y")]
    blocks = over_y + [partner(part) for part in over_y]
    return call(
        final_kernel,
        [((ROWS, SLICE), bf16)],
        *blocks,
        *out_rows,
        scratch=[pltpu.VMEM((8, ROWS, 2 * CH), bf16)],
    )


def solution(mesh):
    finer = Mesh(mesh.devices.reshape(4, 4, 4, 2), ("z", "x", "y", "c"))
    split_specs = P(SP, TP)
    in_specs = (
        split_specs, P(), split_specs, split_specs, P(), P(), P(), P(), P(), P(), P(), P(), P(), P(), split_specs, split_specs,
    )
    return jax.shard_map(body, mesh=finer, in_specs=in_specs, out_specs=split_specs, check_vma=False)
```

```python
import jax
import jax.numpy as jnp
from jax import lax
from jax.experimental import pallas as pl
from jax.experimental.pallas import tpu as pltpu
from jax.sharding import Mesh
from jax.sharding import PartitionSpec as P

SP = ("z", "x")
TP = ("y", "c")
RING = 4
ROWS = 256
WIDTH = 3072
SLICE = 384
LENGTH = 4096
CH = 128
GROUPS = 8
COLS = 512
HALO = 16
epsilon = 1e-06

bf16, f32 = jnp.bfloat16, jnp.float32


def call(body, outs, *args, scratch=(), hbm=(), anywhere=(), limit=8, name=None):
    vmem_spec, hbm_spec = (pl.BlockSpec(memory_space=space) for space in (pltpu.VMEM, pltpu.HBM))
    shapes, out_specs = [], []
    for shape, dtype, *where in outs:
        kind = {"": pltpu.VMEM, "hbm": pltpu.HBM, "last": jax.ShapeDtypeStruct}[where[0] if where else ""]
        shapes.append(kind(shape, dtype))
        out_specs.append(hbm_spec if where == ["hbm"] else vmem_spec)
    held, in_specs = [], []
    for k, arg in enumerate(args):
        if k in anywhere:
            held.append(arg)
            in_specs.append(pl.BlockSpec(memory_space=pl.ANY))
        else:
            held.append(pltpu.with_memory_space_constraint(arg, pltpu.HBM if k in hbm else pltpu.VMEM))
            in_specs.append(hbm_spec if k in hbm else vmem_spec)
    name = name or body.__name__.removesuffix("_kernel")
    single = len(outs) == 1
    return pl.pallas_call(
        body,
        out_shape=shapes[0] if single else shapes,
        in_specs=in_specs,
        out_specs=out_specs[0] if single else out_specs,
        scratch_shapes=list(scratch),
        compiler_params=pltpu.CompilerParams(vmem_limit_bytes=limit << 20),
    )(*held)


def fetch(moves, sems):
    copies = [pltpu.make_async_copy(src, dst, sems.at[k]) for k, (src, dst) in enumerate(moves)]
    for copy in copies:
        copy.start()
    return copies


def arrive(copies):
    for copy in copies:
        copy.wait()


def iota(shape, dim):
    return lax.broadcasted_iota(jnp.int32, shape, dim)


def where_am_i():
    z, x, y, c = (lax.axis_index(a) for a in ("z", "x", "y", "c"))
    return z, x, y, c


def ring(index, back):
    return lax.rem(index + RING - back, RING)


def nt(a, b):
    return lax.dot_general(a, b, (((1,), (1,)), ((), ())), preferred_element_type=f32)


def split(value):
    high = value.astype(bf16)
    return high, (value - high.astype(f32)).astype(bf16)


def pack_kernel(ws, wp, os, op, tokens, gain, rows_in, rows_out, scaled, tokens_v, gain_v, sems):
    copies = fetch(
        [
            (gain, gain_v),
            (tokens, tokens_v),
            (ws, rows_in.at[:, pl.ds(0, CH)]),
            (wp, rows_in.at[:, pl.ds(CH, CH)]),
            (os, rows_out.at[0]),
            (op, rows_out.at[1]),
        ],
        sems,
    )
    t = lax.axis_index("y") * 2 + lax.axis_index("c")
    arrive(copies[:2])
    squares = jnp.zeros((16, ROWS), f32)
    ones = jnp.ones((16, 128), bf16)
    for j in range(3):
        cols = slice(128 * j, 128 * (j + 1))
        value = tokens_v[:, cols].astype(f32)
        scaled[0:ROWS, cols] = (value * gain_v[pl.ds(3 * t + j, 1)]).astype(bf16)
        for part in split(value * value):
            squares += nt(ones, part)
    high = squares.astype(bf16).astype(f32)
    scaled[ROWS:, 0:ROWS] = jnp.where(iota((16, ROWS), 0) < 8, high, squares - high).astype(bf16)
    scaled[ROWS:, ROWS:] = jnp.zeros((16, SLICE - ROWS), bf16)
    arrive(copies[2:])


def join_ring(parts, axis, name, where=()):
    def body(m0, m1, m2, m3, joined, *sems):
        index = lax.axis_index(axis)
        moves = [(m, joined.at[ring(index, k)]) for k, m in enumerate((m0, m1, m2, m3))]
        if sems:
            arrive(fetch(moves, sems[0]))
        else:
            for m, place in moves:
                place[...] = m[...]

    scratch = [pltpu.SemaphoreType.DMA((4,))] if where else []
    return call(body, [((RING, *parts[0].shape), parts[0].dtype, *where)], *parts, scratch=scratch, name=name)


def spread_of(rows):
    return (iota((rows, COLS), 0) % 64 == iota((rows, COLS), 1) % 64).astype(bf16)


def across(value, spread):
    pair = jnp.concatenate(split(value[...].reshape(CH, 64)), axis=1)
    wide = jnp.dot(pair, spread, preferred_element_type=f32)
    return jnp.where(iota((CH, COLS), 0) // 16 == iota((CH, COLS), 1) // 64, wide, 0.0)


def heads_of(array):
    t = lax.axis_index("y") * 2 + lax.axis_index("c")
    return array.at[pl.ds(pl.multiple_of(t * GROUPS, GROUPS), GROUPS)]


def tables_kernel(rr, ri, ls_hbm, inr, ini, d_hbm, t_ref, rr_v, ri_v, inr_v, ini_v, d_ref, ls, sems):
    g0 = (lax.axis_index("y") * 2 + lax.axis_index("c")) * GROUPS
    arrive(fetch([(heads_of(rr), rr_v), (heads_of(ri), ri_v), (heads_of(inr), inr_v), (heads_of(ini), ini_v), (ls_hbm, ls)], sems))

    spread = spread_of(CH)
    own_row = iota((GROUPS, COLS), 1) // 64 == iota((GROUPS, COLS), 0)

    def flat(value):
        high, low = split(value)
        rest = (value - high.astype(f32)) - low.astype(f32)
        wide = jnp.dot(jnp.concatenate([high, low], axis=1), spread, preferred_element_type=f32)
        wide = wide + jnp.dot(rest.astype(bf16), spread[0:64], preferred_element_type=f32)
        return jnp.sum(jnp.where(own_row, wide, 0.0), axis=0, keepdims=True)

    logs = jnp.broadcast_to(ls[...], (GROUPS, 64))
    mine = iota((GROUPS, 64), 1) == iota((GROUPS, 64), 0) + g0
    step = jnp.exp(jnp.sum(jnp.where(mine, logs, 0.0), axis=1, keepdims=True)) / LENGTH
    rate_r, rate_i = flat(rr_v[...]), flat(ri_v[...])
    step = flat(jnp.broadcast_to(step, (GROUPS, 64)))
    exponent, angle = rate_r * step, rate_i * step
    row = iota((8, COLS), 0)
    for first, count in ((0, row + 1), (16, 7 - row)):
        count = count.astype(f32)
        size = jnp.exp(exponent * count)
        t_ref[first : first + 8] = size * jnp.cos(angle * count)
        t_ref[first + 8 : first + 16] = size * jnp.sin(angle * count)
    decay_i = t_ref[8:9]
    grown = exponent * (1.0 + exponent * (0.5 + exponent * (1.0 / 6.0 + exponent * (1.0 / 24.0))))
    half = jnp.sin(0.5 * angle)
    less_one = grown * jnp.cos(angle) - 2.0 * half * half
    below = rate_r * rate_r + rate_i * rate_i
    factor_r = (less_one * rate_r + decay_i * rate_i) / below
    factor_i = (decay_i * rate_r - less_one * rate_i) / below

    in_r, in_i = across(inr_v, spread), across(ini_v, spread)
    for part, value in ((0, factor_r * in_r - factor_i * in_i), (1, factor_r * in_i + factor_i * in_r)):
        high, low = split(value)
        d_ref[0:CH, COLS * part : COLS * (part + 1)] = high
        d_ref[CH : 2 * CH, COLS * part : COLS * (part + 1)] = low
    arrive(fetch([(d_ref, d_hbm)], sems))


def pushes(value, drive, push):
    push[...] = jnp.dot(jnp.concatenate([value, value], axis=1), drive[...], preferred_element_type=f32)


def project_kernel(*refs):
    blocks, weights, drive_hbm, t = refs[:8], refs[8:12], refs[12], refs[13]
    mixed, payload_hbm, payload, total, drive, push, sems = refs[14:]
    z, _, y, c = where_am_i()
    (drive_copy,) = fetch([(drive_hbm, drive)], sems)
    squares = blocks[0][ROWS:, 0:ROWS].astype(f32)
    for block in blocks[1:]:
        squares += block[ROWS:, 0:ROWS].astype(f32)
    squares = jnp.sum(jnp.transpose(squares), axis=1, keepdims=True) * 0.125
    inverse = lax.rsqrt(squares / WIDTH + epsilon)
    gap = lax.rem(y - z + RING, RING)
    for variant in range(RING):

        @pl.when(gap == variant)
        def _():
            value = jnp.zeros((ROWS, 2 * CH), f32)
            for j in range(RING):
                k = (variant + j) % RING
                left = jnp.concatenate([blocks[k][0:ROWS], blocks[k + 4][0:ROWS]], axis=1)
                right = [weights[j][pl.ds(2 * at, 2)].reshape(SLICE, 2 * CH) for at in (c, 1 - c)]
                value += jnp.dot(left, jnp.concatenate(right, axis=0), preferred_element_type=f32)
            total[...] = value

    value = (total[...] * inverse).astype(bf16)
    mixed[...] = value
    drive_copy.wait()
    pushes(value[:, 0:CH], drive, push)
    sums = [(jnp.zeros((8, 128), f32), jnp.zeros((8, 128), f32)) for _ in range(4)]
    for k in range(ROWS // 8):
        for j in range(4):
            at_r, at_i = slice(128 * j, 128 * (j + 1)), slice(COLS + 128 * j, COLS + 128 * (j + 1))
            by_r, by_i = t[7:8, at_r], t[15:16, at_r]
            real, imag = push[8 * k : 8 * k + 8, at_r], push[8 * k : 8 * k + 8, at_i]
            old_r, old_i = sums[j]
            sums[j] = (real + (old_r * by_r - old_i * by_i), imag + (old_r * by_i + old_i * by_r))
    for j, (real, imag) in enumerate(sums):
        cols = slice(128 * j, 128 * (j + 1))
        by_r, by_i = t[16:24, cols], t[24:32, cols]
        payload[j : j + 1] = jnp.sum(real * by_r - imag * by_i, axis=0, keepdims=True)
        payload[4 + j : 5 + j] = jnp.sum(real * by_i + imag * by_r, axis=0, keepdims=True)
    payload[8:24] = value[ROWS - HALO :, CH : 2 * CH].astype(f32)
    arrive(fetch([(payload, payload_hbm.at[peer]) for peer in range(16)], sems))


def local_kernel(
    mixed, drive_hbm, t, outr, outi, pw, skip, gain, keep, r, push, drive, outr_v, outi_v, pw_v, skip_v, gain_v, sems
):
    z, x, y, c = where_am_i()
    s = z * RING + x
    coming = fetch(
        [
            (drive_hbm, drive),
            (heads_of(outr), outr_v),
            (heads_of(outi), outi_v),
            (pw.at[pl.ds((y * 2 + c) * 2, 2)], pw_v),
            (skip, skip_v),
            (gain, gain_v),
        ],
        sems,
    )
    row = iota((8, COLS), 0)
    by_r, by_i = t[7:8], t[15:16]
    for _ in range(5):
        by_r, by_i = by_r * by_r - by_i * by_i, 2.0 * by_r * by_i
    gap = s - 1 - iota((16, COLS), 0)
    real, imag = jnp.where(gap >= 0, 1.0, 0.0), jnp.zeros((16, COLS), f32)
    for bit in range(4):
        on = (jnp.maximum(gap, 0) >> bit) % 2 == 1
        real, imag = (
            jnp.where(on, real * by_r - imag * by_i, real),
            jnp.where(on, real * by_i + imag * by_r, imag),
        )
        by_r, by_i = by_r * by_r - by_i * by_i, 2.0 * by_r * by_i
    keep[ROWS : ROWS + 16, 0:COLS], keep[ROWS : ROWS + 16, COLS:] = real, imag

    coming[0].wait()
    pushes(mixed[:, 0:CH], drive, push)
    for j in range(4):
        at_r, at_i = slice(128 * j, 128 * (j + 1)), slice(COLS + 128 * j, COLS + 128 * (j + 1))
        levels = []
        for by in (1, 2, 4):
            far = row[:, 0:128] >= by
            levels.append((by, jnp.where(far, t[by - 1 : by, at_r], 0.0), jnp.where(far, t[by + 7 : by + 8, at_r], 0.0)))
        for k in range(ROWS // 8):
            rows = slice(8 * k, 8 * k + 8)
            real, imag = push[rows, at_r], push[rows, at_i]
            for by, mul_r, mul_i in levels:
                old_r, old_i = pltpu.roll(real, by, 0), pltpu.roll(imag, by, 0)
                real, imag = real + mul_r * old_r - mul_i * old_i, imag + mul_r * old_i + mul_i * old_r
            keep[rows, at_r] = real
            keep[rows, at_i] = imag

    arrive(coming[1:])
    spread = spread_of(CH)
    for part, (value, sign) in enumerate(((outr_v, 1.0), (outi_v, -1.0))):
        high, low = split(sign * across(value, spread))
        r[0:CH, COLS * part : COLS * (part + 1)] = high
        r[CH : 2 * CH, COLS * part : COLS * (part + 1)] = low
    pick = (iota((64, CH), 0) == iota((64, CH), 1) % 64).astype(bf16)
    wide = jnp.dot(pw_v[...].reshape(CH, 64), pick, preferred_element_type=f32)
    wide = jnp.where(iota((CH, CH), 0) // 64 == iota((CH, CH), 1) // 64, wide, 0.0).astype(bf16)
    r[0:CH, 2 * COLS :] = wide
    r[CH : 2 * CH, 2 * COLS :] = wide
    me = y * 2 + c
    keep[ROWS + 16 : ROWS + 24, 0:128] = jnp.broadcast_to(skip_v[pl.ds(me, 1)], (8, 128))
    keep[ROWS + 16 : ROWS + 24, 128:256] = jnp.broadcast_to(gain_v[pl.ds(me, 1)], (8, 128))


def mix_kernel(x_ref, ends, t, r, mixed, outs, high, low):
    z, x, y, c = where_am_i()
    s = z * RING + x
    me = y * 2 + c
    carries = []
    for j in range(4):
        cols = slice(128 * j, 128 * (j + 1))
        real, imag = ends[:, j, :], ends[:, 4 + j, :]
        at = slice(COLS + 128 * j, COLS + 128 * (j + 1))
        mul_r, mul_i = x_ref[ROWS : ROWS + 16, cols], x_ref[ROWS : ROWS + 16, at]
        carries.append(
            [
                jnp.sum(mul_r * real - mul_i * imag, axis=0, keepdims=True),
                jnp.sum(mul_r * imag + mul_i * real, axis=0, keepdims=True),
            ]
        )
    for k in range(ROWS // 16):
        for j in range(4):
            at_r, at_i = slice(128 * j, 128 * (j + 1)), slice(COLS + 128 * j, COLS + 128 * (j + 1))
            base_r, base_i = t[0:8, at_r], t[8:16, at_r]
            both_r, both_i = [], []
            for h in range(2):
                rows = slice(16 * k + 8 * h, 16 * k + 8 * h + 8)
                old_r, old_i = carries[j]
                real = x_ref[rows, at_r] + (base_r * old_r - base_i * old_i)
                imag = x_ref[rows, at_i] + (base_r * old_i + base_i * old_r)
                carries[j] = [real[7:8], imag[7:8]]
                both_r.append(real)
                both_i.append(imag)
            rows = slice(16 * k, 16 * k + 16)
            for at, both in ((at_r, both_r), (at_i, both_i)):
                high[rows, at], low[rows, at] = split(jnp.concatenate(both, axis=0))
    wide = nt(high[...], r[:, 0 : 2 * COLS])
    total = wide[:, 0:CH] + (wide[:, CH : 2 * CH] + nt(low[...], r[0:CH, 0 : 2 * COLS]))
    total = total + x_ref[ROWS + 16 : ROWS + 17, 0:128] * mixed[:, 0:CH].astype(f32)
    state_out = jax.nn.gelu(total)

    own = mixed[:, CH : 2 * CH].astype(f32)
    halo = jnp.where(s > 0, ends[jnp.maximum(s - 1, 0), 8:24, :], 0.0)
    ext = jnp.concatenate([halo, own], axis=0)
    sums = []
    for k in range(4):
        ext = ext + pltpu.roll(ext, 1 << k, 0)
        sums.append(ext[HALO:])
    lane = iota((ROWS, CH), 1)
    odd = me % 2 == 1
    near = jnp.where(odd, sums[2], sums[0])
    far = jnp.where(odd, sums[3], sums[1])
    window = jnp.where(odd, jnp.where(lane < 64, 8, 16), jnp.where(lane < 64, 2, 4))
    count = jnp.minimum(s * ROWS + 1 + iota((ROWS, CH), 0), window).astype(f32)
    pooled = jnp.where(lane < 64, near, far) / count - own
    pair = jnp.concatenate(split(pooled), axis=1)
    pool_out = jnp.dot(pair, r[:, 2 * COLS :], preferred_element_type=f32) * x_ref[ROWS + 16 : ROWS + 17, 128:256]
    outs[:, 0:CH] = jnp.where(lane < 64, state_out, pltpu.roll(pool_out, 64, 1)).astype(bf16)
    outs[:, CH : 2 * CH] = jnp.where(lane < 64, pltpu.roll(state_out, 64, 1), pool_out).astype(bf16)


def hold_out_kernel(m0, m1, m2, m3, held, sems):
    x = lax.axis_index("x")
    arrive(fetch([(m, held.at[ring(x, k)]) for k, m in enumerate((m0, m1, m2, m3))], sems))


def final_kernel(*refs):
    blocks, weights, out_hbm, held, out, sems = refs[:8], *refs[8:]
    y, c = (lax.axis_index(a) for a in ("y", "c"))
    for k, block in enumerate(blocks):
        from_y, from_c = ring(y, k % 4), c if k < 4 else 1 - c
        for h in range(2):
            held[from_y, from_c * 2 + h] = block[:, CH * h : CH * (h + 1)]
    copies = []
    for h in range(2):
        rows = slice(h * ROWS // 2, (h + 1) * ROWS // 2)
        total = jnp.zeros((ROWS // 2, SLICE), f32)
        for from_x in range(RING):
            for m in (0, 2):
                left = jnp.concatenate([held[m, from_x, rows], held[m + 1, from_x, rows]], axis=1)
                right = weights[from_x, m : m + 2].reshape(2 * CH, SLICE)
                total += jnp.dot(left, right, preferred_element_type=f32)
        out[rows] = total.astype(bf16)
        copies.append(pltpu.make_async_copy(out.at[rows], out_hbm.at[rows], sems.at[h]))
        copies[h].start()
    arrive(copies)


def shift(value, axis, by):
    return lax.ppermute(value, axis, [(i, (i + by) % RING) for i in range(RING)])


def around(value, axis):
    return [value, *(shift(value, axis, k) for k in range(1, RING))]


def partner(value):
    return lax.ppermute(value, "c", [(0, 1), (1, 0)])


def body(
    tokens,
    norm_gain,
    state_in_weight,
    pool_in_weight,
    rate_real,
    rate_imag,
    log_step,
    input_real,
    input_imag,
    output_real,
    output_imag,
    skip_gain,
    pool_weight,
    pool_gain,
    state_out_weight,
    pool_out_weight,
):
    rows_in, rows_out, scaled = call(
        pack_kernel,
        [((192, 2 * CH), bf16), ((2, 64, SLICE), bf16), ((ROWS + 16, SLICE), bf16)],
        state_in_weight,
        pool_in_weight,
        state_out_weight,
        pool_out_weight,
        tokens,
        norm_gain.reshape(24, 128),
        hbm=(0, 1, 2, 3, 4, 5),
        scratch=[pltpu.VMEM((ROWS, SLICE), bf16), pltpu.VMEM((24, 128), f32), pltpu.SemaphoreType.DMA((6,))],
    )
    joined_in = join_ring(around(rows_in, "x"), "x", "join_in")
    in_weights = around(joined_in, "z")
    joined_out = join_ring(around(rows_out, "z"), "z", "join_out")
    out_weights = around(joined_out, "x")
    over_y = around(scaled, "y")
    blocks = over_y + [partner(part) for part in over_y]

    small = [pltpu.VMEM((GROUPS, 64), f32)] * 2 + [pltpu.VMEM((GROUPS, 16, 64), f32)] * 2
    drive, table = call(
        tables_kernel,
        [((2 * CH, 2 * COLS), bf16, "hbm"), ((32, COLS), f32)],
        rate_real,
        rate_imag,
        log_step.reshape(1, 64),
        input_real.swapaxes(1, 2),
        input_imag.swapaxes(1, 2),
        hbm=(0, 1, 2, 3, 4),
        scratch=[
            *small,
            pltpu.VMEM((2 * CH, 2 * COLS), bf16),
            pltpu.VMEM((1, 64), f32),
            pltpu.SemaphoreType.DMA((5,)),
        ],
    )
    mixed, payload = call(
        project_kernel,
        [((ROWS, 2 * CH), bf16), ((16, 24, 128), f32, "hbm")],
        *blocks,
        *in_weights,
        drive,
        table,
        hbm=(12,),
        scratch=[
            pltpu.VMEM((24, 128), f32),
            pltpu.VMEM((ROWS, 2 * CH), f32),
            pltpu.VMEM((2 * CH, 2 * COLS), bf16),
            pltpu.VMEM((ROWS, 2 * COLS), f32),
            pltpu.SemaphoreType.DMA((16,)),
        ],
    )
    ends = lax.all_to_all(payload, SP, 0, 0, tiled=True)
    local, read = call(
        local_kernel,
        [((ROWS + 24, 2 * COLS), f32), ((2 * CH, 2 * COLS + CH), bf16)],
        mixed,
        drive,
        table,
        output_real,
        output_imag,
        pool_weight,
        skip_gain.reshape(8, 128),
        pool_gain.reshape(8, 128),
        hbm=(1, 3, 4, 5, 6, 7),
        scratch=[
            pltpu.VMEM((ROWS, 2 * COLS), f32),
            pltpu.VMEM((2 * CH, 2 * COLS), bf16),
            *small[2:],
            pltpu.VMEM((2, 64, 64), bf16),
            pltpu.VMEM((8, 128), f32),
            pltpu.VMEM((8, 128), f32),
            pltpu.SemaphoreType.DMA((6,)),
        ],
    )
    outs = call(
        mix_kernel,
        [((ROWS, 2 * CH), bf16)],
        local,
        ends,
        table,
        read,
        mixed,
        scratch=[pltpu.VMEM((ROWS, 2 * COLS), bf16), pltpu.VMEM((ROWS, 2 * COLS), bf16)],
    )
    over_y = around(outs, "y")
    over_c = [partner(part) for part in over_y]
    weights = call(
        hold_out_kernel,
        [((RING, RING, 2, 64, SLICE), bf16)],
        *out_weights,
        anywhere=(0, 1, 2, 3),
        scratch=[pltpu.SemaphoreType.DMA((4,))],
    )
    return call(
        final_kernel,
        [((ROWS, SLICE), bf16, "hbm")],
        *over_y,
        *over_c,
        weights,
        scratch=[
            pltpu.VMEM((RING, RING, ROWS, CH), bf16),
            pltpu.VMEM((ROWS, SLICE), bf16),
            pltpu.SemaphoreType.DMA((2,)),
        ],
    )


def solution(mesh):
    finer = Mesh(mesh.devices.reshape(4, 4, 4, 2), ("z", "x", "y", "c"))
    split_specs = P(SP, TP)
    in_specs = (
        split_specs, P(), split_specs, split_specs, P(), P(), P(), P(), P(), P(), P(), P(), P(), P(), split_specs, split_specs,
    )

    return jax.shard_map(body, mesh=finer, in_specs=in_specs, out_specs=split_specs, check_vma=False)
```

```python
import jax
import jax.numpy as jnp
from jax import lax
from jax.experimental import pallas as pl
from jax.experimental.pallas import tpu as pltpu
from jax.sharding import Mesh
from jax.sharding import PartitionSpec as P

SP = ("z", "x")
TP = ("y", "c")
RING = 4
ROWS = 256
WIDTH = 3072
SLICE = 384
LENGTH = 4096
CH = 128
GROUPS = 8
COLS = 512
HALO = 16
epsilon = 1e-06

bf16, f32 = jnp.bfloat16, jnp.float32


def call(body, outs, *args, scratch=(), hbm=(), anywhere=(), limit=8, name=None):
    vmem_spec, hbm_spec = (pl.BlockSpec(memory_space=space) for space in (pltpu.VMEM, pltpu.HBM))
    shapes, out_specs = [], []
    for shape, dtype, *where in outs:
        kind = {"": pltpu.VMEM, "hbm": pltpu.HBM, "last": jax.ShapeDtypeStruct}[where[0] if where else ""]
        shapes.append(kind(shape, dtype))
        out_specs.append(hbm_spec if where == ["hbm"] else vmem_spec)
    held, in_specs = [], []
    for k, arg in enumerate(args):
        if k in anywhere:
            held.append(arg)
            in_specs.append(pl.BlockSpec(memory_space=pl.ANY))
        else:
            held.append(pltpu.with_memory_space_constraint(arg, pltpu.HBM if k in hbm else pltpu.VMEM))
            in_specs.append(hbm_spec if k in hbm else vmem_spec)
    name = name or body.__name__.removesuffix("_kernel")
    single = len(outs) == 1
    return pl.pallas_call(
        body,
        out_shape=shapes[0] if single else shapes,
        in_specs=in_specs,
        out_specs=out_specs[0] if single else out_specs,
        scratch_shapes=list(scratch),
        compiler_params=pltpu.CompilerParams(vmem_limit_bytes=limit << 20),
    )(*held)


def fetch(moves, sems):
    copies = [pltpu.make_async_copy(src, dst, sems.at[k]) for k, (src, dst) in enumerate(moves)]
    for copy in copies:
        copy.start()
    return copies


def arrive(copies):
    for copy in copies:
        copy.wait()


def iota(shape, dim):
    return lax.broadcasted_iota(jnp.int32, shape, dim)


def where_am_i():
    z, x, y, c = (lax.axis_index(a) for a in ("z", "x", "y", "c"))
    return z, x, y, c


def ring(index, back):
    return lax.rem(index + RING - back, RING)


def nt(a, b):
    return lax.dot_general(a, b, (((1,), (1,)), ((), ())), preferred_element_type=f32)


def split(value):
    high = value.astype(bf16)
    return high, (value - high.astype(f32)).astype(bf16)


def pack_kernel(ws, wp, os, op, tokens, gain, rows_in, rows_out, scaled, tokens_v, gain_v, sems):
    copies = fetch(
        [
            (gain, gain_v),
            (tokens, tokens_v),
            (ws, rows_in.at[:, pl.ds(0, CH)]),
            (wp, rows_in.at[:, pl.ds(CH, CH)]),
            (os, rows_out.at[0]),
            (op, rows_out.at[1]),
        ],
        sems,
    )
    t = lax.axis_index("y") * 2 + lax.axis_index("c")
    arrive(copies[:2])
    squares = jnp.zeros((16, ROWS), f32)
    ones = jnp.ones((16, 128), bf16)
    for j in range(3):
        cols = slice(128 * j, 128 * (j + 1))
        value = tokens_v[:, cols].astype(f32)
        scaled[0:ROWS, cols] = (value * gain_v[pl.ds(3 * t + j, 1)]).astype(bf16)
        for part in split(value * value):
            squares += nt(ones, part)
    high = squares.astype(bf16).astype(f32)
    scaled[ROWS:, 0:ROWS] = jnp.where(iota((16, ROWS), 0) < 8, high, squares - high).astype(bf16)
    scaled[ROWS:, ROWS:] = jnp.zeros((16, SLICE - ROWS), bf16)
    arrive(copies[2:])


def axis_index_of(which):
    x, z = lax.axis_index("x"), lax.axis_index("z")
    return jnp.where(lax.axis_index("c") == which, x, z)


def join_ring(parts, which, name):
    def body(m0, m1, m2, m3, joined):
        index = axis_index_of(which)
        for k, m in enumerate((m0, m1, m2, m3)):
            joined[ring(index, k)] = m[...]

    return call(body, [((RING, *parts[0].shape), parts[0].dtype)], *parts, name=name)


def spread_of(rows):
    return (iota((rows, COLS), 0) % 64 == iota((rows, COLS), 1) % 64).astype(bf16)


def across(value, spread):
    pair = jnp.concatenate(split(value[...].reshape(CH, 64)), axis=1)
    wide = jnp.dot(pair, spread, preferred_element_type=f32)
    return jnp.where(iota((CH, COLS), 0) // 16 == iota((CH, COLS), 1) // 64, wide, 0.0)


def heads_of(array):
    t = lax.axis_index("y") * 2 + lax.axis_index("c")
    return array.at[pl.ds(pl.multiple_of(t * GROUPS, GROUPS), GROUPS)]


def tables_kernel(rr, ri, ls_hbm, inr, ini, d_hbm, t_ref, rr_v, ri_v, inr_v, ini_v, d_ref, ls, sems):
    g0 = (lax.axis_index("y") * 2 + lax.axis_index("c")) * GROUPS
    arrive(fetch([(heads_of(rr), rr_v), (heads_of(ri), ri_v), (heads_of(inr), inr_v), (heads_of(ini), ini_v), (ls_hbm, ls)], sems))

    spread = spread_of(CH)
    own_row = iota((GROUPS, COLS), 1) // 64 == iota((GROUPS, COLS), 0)

    def flat(value):
        high, low = split(value)
        rest = (value - high.astype(f32)) - low.astype(f32)
        wide = jnp.dot(jnp.concatenate([high, low], axis=1), spread, preferred_element_type=f32)
        wide = wide + jnp.dot(rest.astype(bf16), spread[0:64], preferred_element_type=f32)
        return jnp.sum(jnp.where(own_row, wide, 0.0), axis=0, keepdims=True)

    logs = jnp.broadcast_to(ls[...], (GROUPS, 64))
    mine = iota((GROUPS, 64), 1) == iota((GROUPS, 64), 0) + g0
    step = jnp.exp(jnp.sum(jnp.where(mine, logs, 0.0), axis=1, keepdims=True)) / LENGTH
    rate_r, rate_i = flat(rr_v[...]), flat(ri_v[...])
    step = flat(jnp.broadcast_to(step, (GROUPS, 64)))
    exponent, angle = rate_r * step, rate_i * step
    row = iota((8, COLS), 0)
    for first, count in ((0, row + 1), (16, 7 - row)):
        count = count.astype(f32)
        size = jnp.exp(exponent * count)
        t_ref[first : first + 8] = size * jnp.cos(angle * count)
        t_ref[first + 8 : first + 16] = size * jnp.sin(angle * count)
    decay_i = t_ref[8:9]
    grown = exponent * (1.0 + exponent * (0.5 + exponent * (1.0 / 6.0 + exponent * (1.0 / 24.0))))
    half = jnp.sin(0.5 * angle)
    less_one = grown * jnp.cos(angle) - 2.0 * half * half
    below = rate_r * rate_r + rate_i * rate_i
    factor_r = (less_one * rate_r + decay_i * rate_i) / below
    factor_i = (decay_i * rate_r - less_one * rate_i) / below

    in_r, in_i = across(inr_v, spread), across(ini_v, spread)
    for part, value in ((0, factor_r * in_r - factor_i * in_i), (1, factor_r * in_i + factor_i * in_r)):
        high, low = split(value)
        d_ref[0:CH, COLS * part : COLS * (part + 1)] = high
        d_ref[CH : 2 * CH, COLS * part : COLS * (part + 1)] = low
    arrive(fetch([(d_ref, d_hbm)], sems))


def pushes(value, drive, push):
    push[...] = jnp.dot(jnp.concatenate([value, value], axis=1), drive[...], preferred_element_type=f32)


def project_kernel(*refs):
    blocks, weights, drive_hbm, t = refs[:8], refs[8:12], refs[12], refs[13]
    mixed, payload_hbm, payload, ordered, drive, push, sems = refs[14:]
    z, x, y, c = where_am_i()
    (drive_copy,) = fetch([(drive_hbm, drive)], sems)
    squares = blocks[0][ROWS:, 0:ROWS].astype(f32)
    for block in blocks[1:]:
        squares += block[ROWS:, 0:ROWS].astype(f32)
    squares = jnp.sum(jnp.transpose(squares), axis=1, keepdims=True) * 0.125
    inverse = lax.rsqrt(squares / WIDTH + epsilon)
    for k in range(RING):
        for u in range(RING):
            from_z, from_x = jnp.where(c == 0, ring(z, k), u), jnp.where(c == 0, u, ring(x, k))
            ordered[from_z, from_x] = weights[k][u]
    total = jnp.zeros((ROWS, 2 * CH), f32)
    for k in range(RING):
        at = ring(y, k)
        left = jnp.concatenate([blocks[k][0:ROWS], blocks[k + 4][0:ROWS]], axis=1)
        right = [ordered[at, pl.ds(2 * core, 2)].reshape(SLICE, 2 * CH) for core in (c, 1 - c)]
        total += jnp.dot(left, jnp.concatenate(right, axis=0), preferred_element_type=f32)
    value = (total * inverse).astype(bf16)
    mixed[...] = value
    drive_copy.wait()
    pushes(value[:, 0:CH], drive, push)
    sums = [(jnp.zeros((8, 128), f32), jnp.zeros((8, 128), f32)) for _ in range(4)]
    for k in range(ROWS // 8):
        for j in range(4):
            at_r, at_i = slice(128 * j, 128 * (j + 1)), slice(COLS + 128 * j, COLS + 128 * (j + 1))
            by_r, by_i = t[7:8, at_r], t[15:16, at_r]
            real, imag = push[8 * k : 8 * k + 8, at_r], push[8 * k : 8 * k + 8, at_i]
            old_r, old_i = sums[j]
            sums[j] = (real + (old_r * by_r - old_i * by_i), imag + (old_r * by_i + old_i * by_r))
    for j, (real, imag) in enumerate(sums):
        cols = slice(128 * j, 128 * (j + 1))
        by_r, by_i = t[16:24, cols], t[24:32, cols]
        payload[j : j + 1] = jnp.sum(real * by_r - imag * by_i, axis=0, keepdims=True)
        payload[4 + j : 5 + j] = jnp.sum(real * by_i + imag * by_r, axis=0, keepdims=True)
    payload[8:24] = value[ROWS - HALO :, CH : 2 * CH].astype(f32)
    arrive(fetch([(payload, payload_hbm.at[peer]) for peer in range(16)], sems))


def local_kernel(
    mixed, drive_hbm, t, outr, outi, pw, skip, gain, keep, r, push, drive, outr_v, outi_v, pw_v, skip_v, gain_v, sems
):
    z, x, y, c = where_am_i()
    s = z * RING + x
    coming = fetch(
        [
            (drive_hbm, drive),
            (heads_of(outr), outr_v),
            (heads_of(outi), outi_v),
            (pw.at[pl.ds((y * 2 + c) * 2, 2)], pw_v),
            (skip, skip_v),
            (gain, gain_v),
        ],
        sems,
    )
    row = iota((8, COLS), 0)
    by_r, by_i = t[7:8], t[15:16]
    for _ in range(5):
        by_r, by_i = by_r * by_r - by_i * by_i, 2.0 * by_r * by_i
    gap = s - 1 - iota((16, COLS), 0)
    real, imag = jnp.where(gap >= 0, 1.0, 0.0), jnp.zeros((16, COLS), f32)
    for bit in range(4):
        on = (jnp.maximum(gap, 0) >> bit) % 2 == 1
        real, imag = (
            jnp.where(on, real * by_r - imag * by_i, real),
            jnp.where(on, real * by_i + imag * by_r, imag),
        )
        by_r, by_i = by_r * by_r - by_i * by_i, 2.0 * by_r * by_i
    keep[ROWS : ROWS + 16, 0:COLS], keep[ROWS : ROWS + 16, COLS:] = real, imag

    coming[0].wait()
    pushes(mixed[:, 0:CH], drive, push)
    for j in range(4):
        at_r, at_i = slice(128 * j, 128 * (j + 1)), slice(COLS + 128 * j, COLS + 128 * (j + 1))
        levels = []
        for by in (1, 2, 4):
            far = row[:, 0:128] >= by
            levels.append((by, jnp.where(far, t[by - 1 : by, at_r], 0.0), jnp.where(far, t[by + 7 : by + 8, at_r], 0.0)))
        for k in range(ROWS // 8):
            rows = slice(8 * k, 8 * k + 8)
            real, imag = push[rows, at_r], push[rows, at_i]
            for by, mul_r, mul_i in levels:
                old_r, old_i = pltpu.roll(real, by, 0), pltpu.roll(imag, by, 0)
                real, imag = real + mul_r * old_r - mul_i * old_i, imag + mul_r * old_i + mul_i * old_r
            keep[rows, at_r] = real
            keep[rows, at_i] = imag

    arrive(coming[1:])
    spread = spread_of(CH)
    for part, (value, sign) in enumerate(((outr_v, 1.0), (outi_v, -1.0))):
        high, low = split(sign * across(value, spread))
        r[0:CH, COLS * part : COLS * (part + 1)] = high
        r[CH : 2 * CH, COLS * part : COLS * (part + 1)] = low
    pick = (iota((64, CH), 0) == iota((64, CH), 1) % 64).astype(bf16)
    wide = jnp.dot(pw_v[...].reshape(CH, 64), pick, preferred_element_type=f32)
    wide = jnp.where(iota((CH, CH), 0) // 64 == iota((CH, CH), 1) // 64, wide, 0.0).astype(bf16)
    r[0:CH, 2 * COLS :] = wide
    r[CH : 2 * CH, 2 * COLS :] = wide
    me = y * 2 + c
    keep[ROWS + 16 : ROWS + 24, 0:128] = jnp.broadcast_to(skip_v[pl.ds(me, 1)], (8, 128))
    keep[ROWS + 16 : ROWS + 24, 128:256] = jnp.broadcast_to(gain_v[pl.ds(me, 1)], (8, 128))


def mix_kernel(x_ref, ends, t, r, mixed, outs, high, low):
    z, x, y, c = where_am_i()
    s = z * RING + x
    me = y * 2 + c
    carries = []
    for j in range(4):
        cols = slice(128 * j, 128 * (j + 1))
        real, imag = ends[:, j, :], ends[:, 4 + j, :]
        at = slice(COLS + 128 * j, COLS + 128 * (j + 1))
        mul_r, mul_i = x_ref[ROWS : ROWS + 16, cols], x_ref[ROWS : ROWS + 16, at]
        carries.append(
            [
                jnp.sum(mul_r * real - mul_i * imag, axis=0, keepdims=True),
                jnp.sum(mul_r * imag + mul_i * real, axis=0, keepdims=True),
            ]
        )
    for k in range(ROWS // 16):
        for j in range(4):
            at_r, at_i = slice(128 * j, 128 * (j + 1)), slice(COLS + 128 * j, COLS + 128 * (j + 1))
            base_r, base_i = t[0:8, at_r], t[8:16, at_r]
            both_r, both_i = [], []
            for h in range(2):
                rows = slice(16 * k + 8 * h, 16 * k + 8 * h + 8)
                old_r, old_i = carries[j]
                real = x_ref[rows, at_r] + (base_r * old_r - base_i * old_i)
                imag = x_ref[rows, at_i] + (base_r * old_i + base_i * old_r)
                carries[j] = [real[7:8], imag[7:8]]
                both_r.append(real)
                both_i.append(imag)
            rows = slice(16 * k, 16 * k + 16)
            for at, both in ((at_r, both_r), (at_i, both_i)):
                high[rows, at], low[rows, at] = split(jnp.concatenate(both, axis=0))
    wide = nt(high[...], r[:, 0 : 2 * COLS])
    total = wide[:, 0:CH] + (wide[:, CH : 2 * CH] + nt(low[...], r[0:CH, 0 : 2 * COLS]))
    total = total + x_ref[ROWS + 16 : ROWS + 17, 0:128] * mixed[:, 0:CH].astype(f32)
    state_out = jax.nn.gelu(total)

    own = mixed[:, CH : 2 * CH].astype(f32)
    halo = jnp.where(s > 0, ends[jnp.maximum(s - 1, 0), 8:24, :], 0.0)
    ext = jnp.concatenate([halo, own], axis=0)
    sums = []
    for k in range(4):
        ext = ext + pltpu.roll(ext, 1 << k, 0)
        sums.append(ext[HALO:])
    lane = iota((ROWS, CH), 1)
    odd = me % 2 == 1
    near = jnp.where(odd, sums[2], sums[0])
    far = jnp.where(odd, sums[3], sums[1])
    window = jnp.where(odd, jnp.where(lane < 64, 8, 16), jnp.where(lane < 64, 2, 4))
    count = jnp.minimum(s * ROWS + 1 + iota((ROWS, CH), 0), window).astype(f32)
    pooled = jnp.where(lane < 64, near, far) / count - own
    pair = jnp.concatenate(split(pooled), axis=1)
    pool_out = jnp.dot(pair, r[:, 2 * COLS :], preferred_element_type=f32) * x_ref[ROWS + 16 : ROWS + 17, 128:256]
    outs[:, 0:CH] = jnp.where(lane < 64, state_out, pltpu.roll(pool_out, 64, 1)).astype(bf16)
    outs[:, CH : 2 * CH] = jnp.where(lane < 64, pltpu.roll(state_out, 64, 1), pool_out).astype(bf16)


def hold_out_kernel(m0, m1, m2, m3, held, sems):
    z, x, c = (lax.axis_index(a) for a in ("z", "x", "c"))

    def copies(core):
        places = [held.at[ring(x, k)] if core == 0 else held.at[:, ring(z, k)] for k in range(RING)]
        return [
            pltpu.make_async_copy(m, place, sems.at[k])
            for k, (m, place) in enumerate(zip((m0, m1, m2, m3), places))
        ]

    for core in range(2):

        @pl.when(c == core)
        def _(core=core):
            started = copies(core)
            for copy in started:
                copy.start()
            arrive(started)


def block_products(blocks, from_c, weights, rows):
    y = lax.axis_index("y")
    total = None
    for k, block in enumerate(blocks):
        right = [weights[from_c * 2 + h, ring(y, k)].reshape(CH, SLICE) for h in range(2)]
        part = jnp.dot(block[rows], jnp.concatenate(right, axis=0), preferred_element_type=f32)
        total = part if total is None else total + part
    return total


def direct_kernel(b0, b1, b2, b3, weights, total):
    total[...] = block_products((b0, b1, b2, b3), lax.axis_index("c"), weights, slice(0, ROWS))


def final_kernel(b0, b1, b2, b3, weights, total, out_hbm, out, sems):
    copies = []
    for h in range(2):
        rows = slice(h * ROWS // 2, (h + 1) * ROWS // 2)
        value = total[rows] + block_products((b0, b1, b2, b3), 1 - lax.axis_index("c"), weights, rows)
        out[rows] = value.astype(bf16)
        copies.append(pltpu.make_async_copy(out.at[rows], out_hbm.at[rows], sems.at[h]))
        copies[h].start()
    arrive(copies)


def shift(value, axis, by):
    return lax.ppermute(value, axis, [(i, (i + by) % RING) for i in range(RING)])


def around(value, axis):
    return [value, *(shift(value, axis, k) for k in range(1, RING))]


def along(value, which):
    parts = [value]
    for by in range(1, RING):
        pairs = []
        for z in range(RING):
            for x in range(RING):
                for c in range(2):
                    to_z, to_x = (z, (x + by) % RING) if which == c else ((z + by) % RING, x)
                    pairs.append(((z * RING + x) * 2 + c, (to_z * RING + to_x) * 2 + c))
        parts.append(lax.ppermute(value, ("z", "x", "c"), pairs))
    return parts


def partner(value):
    return lax.ppermute(value, "c", [(0, 1), (1, 0)])


def body(
    tokens,
    norm_gain,
    state_in_weight,
    pool_in_weight,
    rate_real,
    rate_imag,
    log_step,
    input_real,
    input_imag,
    output_real,
    output_imag,
    skip_gain,
    pool_weight,
    pool_gain,
    state_out_weight,
    pool_out_weight,
):
    rows_in, rows_out, scaled = call(
        pack_kernel,
        [((192, 2 * CH), bf16), ((2, 64, SLICE), bf16), ((ROWS + 16, SLICE), bf16)],
        state_in_weight,
        pool_in_weight,
        state_out_weight,
        pool_out_weight,
        tokens,
        norm_gain.reshape(24, 128),
        hbm=(0, 1, 2, 3, 4, 5),
        scratch=[pltpu.VMEM((ROWS, SLICE), bf16), pltpu.VMEM((24, 128), f32), pltpu.SemaphoreType.DMA((6,))],
    )
    joined_in = join_ring(along(rows_in, 0), 0, "join_in")
    in_weights = along(joined_in, 1)
    joined_out = join_ring(along(rows_out, 1), 1, "join_out")
    out_weights = along(joined_out, 0)
    over_y = around(scaled, "y")
    blocks = over_y + [partner(part) for part in over_y]

    small = [pltpu.VMEM((GROUPS, 64), f32)] * 2 + [pltpu.VMEM((GROUPS, 16, 64), f32)] * 2
    drive, table = call(
        tables_kernel,
        [((2 * CH, 2 * COLS), bf16, "hbm"), ((32, COLS), f32)],
        rate_real,
        rate_imag,
        log_step.reshape(1, 64),
        input_real.swapaxes(1, 2),
        input_imag.swapaxes(1, 2),
        hbm=(0, 1, 2, 3, 4),
        scratch=[
            *small,
            pltpu.VMEM((2 * CH, 2 * COLS), bf16),
            pltpu.VMEM((1, 64), f32),
            pltpu.SemaphoreType.DMA((5,)),
        ],
    )
    mixed, payload = call(
        project_kernel,
        [((ROWS, 2 * CH), bf16), ((16, 24, 128), f32, "hbm")],
        *blocks,
        *in_weights,
        drive,
        table,
        hbm=(12,),
        scratch=[
            pltpu.VMEM((24, 128), f32),
            pltpu.VMEM((RING, RING, 192, 2 * CH), bf16),
            pltpu.VMEM((2 * CH, 2 * COLS), bf16),
            pltpu.VMEM((ROWS, 2 * COLS), f32),
            pltpu.SemaphoreType.DMA((16,)),
        ],
    )
    ends = lax.all_to_all(payload, SP, 0, 0, tiled=True)
    local, read = call(
        local_kernel,
        [((ROWS + 24, 2 * COLS), f32), ((2 * CH, 2 * COLS + CH), bf16)],
        mixed,
        drive,
        table,
        output_real,
        output_imag,
        pool_weight,
        skip_gain.reshape(8, 128),
        pool_gain.reshape(8, 128),
        hbm=(1, 3, 4, 5, 6, 7),
        scratch=[
            pltpu.VMEM((ROWS, 2 * COLS), f32),
            pltpu.VMEM((2 * CH, 2 * COLS), bf16),
            *small[2:],
            pltpu.VMEM((2, 64, 64), bf16),
            pltpu.VMEM((8, 128), f32),
            pltpu.VMEM((8, 128), f32),
            pltpu.SemaphoreType.DMA((6,)),
        ],
    )
    outs = call(
        mix_kernel,
        [((ROWS, 2 * CH), bf16)],
        local,
        ends,
        table,
        read,
        mixed,
        scratch=[pltpu.VMEM((ROWS, 2 * COLS), bf16), pltpu.VMEM((ROWS, 2 * COLS), bf16)],
    )
    over_y = around(outs, "y")
    over_c = [partner(part) for part in over_y]
    weights = call(
        hold_out_kernel,
        [((RING, RING, 2, 64, SLICE), bf16)],
        *out_weights,
        anywhere=(0, 1, 2, 3),
        scratch=[pltpu.SemaphoreType.DMA((4,))],
    )
    total = call(direct_kernel, [((ROWS, SLICE), f32)], *over_y, weights)
    return call(
        final_kernel,
        [((ROWS, SLICE), bf16, "hbm")],
        *over_c,
        weights,
        total,
        scratch=[pltpu.VMEM((ROWS, SLICE), bf16), pltpu.SemaphoreType.DMA((2,))],
    )


def solution(mesh):
    finer = Mesh(mesh.devices.reshape(4, 4, 4, 2), ("z", "x", "y", "c"))
    split_specs = P(SP, TP)
    in_specs = (
        split_specs, P(), split_specs, split_specs, P(), P(), P(), P(), P(), P(), P(), P(), P(), P(), split_specs, split_specs,
    )

    return jax.shard_map(body, mesh=finer, in_specs=in_specs, out_specs=split_specs, check_vma=False)
```

```python
import jax
import jax.numpy as jnp
from jax import lax
from jax.experimental import pallas as pl
from jax.experimental.pallas import tpu as pltpu
from jax.sharding import Mesh
from jax.sharding import PartitionSpec as P

SP = ("z", "x")
TP = ("y", "c")
RING = 4
ROWS = 256
WIDTH = 3072
SLICE = 384
LENGTH = 4096
CH = 128
GROUPS = 8
COLS = 512
HALO = 16
epsilon = 1e-06

bf16, f32 = jnp.bfloat16, jnp.float32


def call(body, outs, *args, scratch=(), hbm=(), anywhere=(), limit=8, name=None):
    vmem_spec, hbm_spec = (pl.BlockSpec(memory_space=space) for space in (pltpu.VMEM, pltpu.HBM))
    shapes, out_specs = [], []
    for shape, dtype, *where in outs:
        kind = {"": pltpu.VMEM, "hbm": pltpu.HBM, "last": jax.ShapeDtypeStruct}[where[0] if where else ""]
        shapes.append(kind(shape, dtype))
        out_specs.append(hbm_spec if where == ["hbm"] else vmem_spec)
    held, in_specs = [], []
    for k, arg in enumerate(args):
        if k in anywhere:
            held.append(arg)
            in_specs.append(pl.BlockSpec(memory_space=pl.ANY))
        else:
            held.append(pltpu.with_memory_space_constraint(arg, pltpu.HBM if k in hbm else pltpu.VMEM))
            in_specs.append(hbm_spec if k in hbm else vmem_spec)
    name = name or body.__name__.removesuffix("_kernel")
    single = len(outs) == 1
    return pl.pallas_call(
        body,
        out_shape=shapes[0] if single else shapes,
        in_specs=in_specs,
        out_specs=out_specs[0] if single else out_specs,
        scratch_shapes=list(scratch),
        compiler_params=pltpu.CompilerParams(vmem_limit_bytes=limit << 20),
    )(*held)


def fetch(moves, sems):
    copies = [pltpu.make_async_copy(src, dst, sems.at[k]) for k, (src, dst) in enumerate(moves)]
    for copy in copies:
        copy.start()
    return copies


def arrive(copies):
    for copy in copies:
        copy.wait()


def iota(shape, dim):
    return lax.broadcasted_iota(jnp.int32, shape, dim)


def where_am_i():
    z, x, y, c = (lax.axis_index(a) for a in ("z", "x", "y", "c"))
    return z, x, y, c


def ring(index, back):
    return lax.rem(index + RING - back, RING)


def nt(a, b):
    return lax.dot_general(a, b, (((1,), (1,)), ((), ())), preferred_element_type=f32)


def split(value):
    high = value.astype(bf16)
    return high, (value - high.astype(f32)).astype(bf16)


def pack_kernel(ws, wp, os, op, tokens, gain, rows_in, rows_out, scaled, tokens_v, gain_v, sems):
    copies = fetch(
        [
            (gain, gain_v),
            (tokens, tokens_v),
            (ws, rows_in.at[:, pl.ds(0, CH)]),
            (wp, rows_in.at[:, pl.ds(CH, CH)]),
            (os, rows_out.at[0]),
            (op, rows_out.at[1]),
        ],
        sems,
    )
    t = lax.axis_index("y") * 2 + lax.axis_index("c")
    arrive(copies[:2])
    squares = jnp.zeros((16, ROWS), f32)
    ones = jnp.ones((16, 128), bf16)
    for j in range(3):
        cols = slice(128 * j, 128 * (j + 1))
        value = tokens_v[:, cols].astype(f32)
        scaled[0:ROWS, cols] = (value * gain_v[pl.ds(3 * t + j, 1)]).astype(bf16)
        for part in split(value * value):
            squares += nt(ones, part)
    high = squares.astype(bf16).astype(f32)
    scaled[ROWS:, 0:ROWS] = jnp.where(iota((16, ROWS), 0) < 8, high, squares - high).astype(bf16)
    scaled[ROWS:, ROWS:] = jnp.zeros((16, SLICE - ROWS), bf16)
    arrive(copies[2:])


def axis_index_of(which):
    x, z = lax.axis_index("x"), lax.axis_index("z")
    return jnp.where(lax.axis_index("c") == which, x, z)


def join_ring(parts, which, name):
    def body(m0, m1, m2, m3, joined):
        index = axis_index_of(which)
        for k, m in enumerate((m0, m1, m2, m3)):
            joined[ring(index, k)] = m[...]

    return call(body, [((RING, *parts[0].shape), parts[0].dtype)], *parts, name=name)


def spread_of(rows):
    return (iota((rows, COLS), 0) % 64 == iota((rows, COLS), 1) % 64).astype(bf16)


def across(value, spread):
    pair = jnp.concatenate(split(value[...].reshape(CH, 64)), axis=1)
    wide = jnp.dot(pair, spread, preferred_element_type=f32)
    return jnp.where(iota((CH, COLS), 0) // 16 == iota((CH, COLS), 1) // 64, wide, 0.0)


def heads_of(array):
    t = lax.axis_index("y") * 2 + lax.axis_index("c")
    return array.at[pl.ds(pl.multiple_of(t * GROUPS, GROUPS), GROUPS)]


def tables_kernel(rr, ri, ls_hbm, inr, ini, d_hbm, t_ref, rr_v, ri_v, inr_v, ini_v, d_ref, ls, sems):
    g0 = (lax.axis_index("y") * 2 + lax.axis_index("c")) * GROUPS
    arrive(fetch([(heads_of(rr), rr_v), (heads_of(ri), ri_v), (heads_of(inr), inr_v), (heads_of(ini), ini_v), (ls_hbm, ls)], sems))

    spread = spread_of(CH)
    own_row = iota((GROUPS, COLS), 1) // 64 == iota((GROUPS, COLS), 0)

    def flat(value):
        high, low = split(value)
        rest = (value - high.astype(f32)) - low.astype(f32)
        wide = jnp.dot(jnp.concatenate([high, low], axis=1), spread, preferred_element_type=f32)
        wide = wide + jnp.dot(rest.astype(bf16), spread[0:64], preferred_element_type=f32)
        return jnp.sum(jnp.where(own_row, wide, 0.0), axis=0, keepdims=True)

    logs = jnp.broadcast_to(ls[...], (GROUPS, 64))
    mine = iota((GROUPS, 64), 1) == iota((GROUPS, 64), 0) + g0
    step = jnp.exp(jnp.sum(jnp.where(mine, logs, 0.0), axis=1, keepdims=True)) / LENGTH
    rate_r, rate_i = flat(rr_v[...]), flat(ri_v[...])
    step = flat(jnp.broadcast_to(step, (GROUPS, 64)))
    exponent, angle = rate_r * step, rate_i * step
    row = iota((8, COLS), 0)
    for first, count in ((0, row + 1), (16, 7 - row)):
        count = count.astype(f32)
        size = jnp.exp(exponent * count)
        t_ref[first : first + 8] = size * jnp.cos(angle * count)
        t_ref[first + 8 : first + 16] = size * jnp.sin(angle * count)
    decay_i = t_ref[8:9]
    grown = exponent * (1.0 + exponent * (0.5 + exponent * (1.0 / 6.0 + exponent * (1.0 / 24.0))))
    half = jnp.sin(0.5 * angle)
    less_one = grown * jnp.cos(angle) - 2.0 * half * half
    below = rate_r * rate_r + rate_i * rate_i
    factor_r = (less_one * rate_r + decay_i * rate_i) / below
    factor_i = (decay_i * rate_r - less_one * rate_i) / below

    in_r, in_i = across(inr_v, spread), across(ini_v, spread)
    for part, value in ((0, factor_r * in_r - factor_i * in_i), (1, factor_r * in_i + factor_i * in_r)):
        high, low = split(value)
        d_ref[0:CH, COLS * part : COLS * (part + 1)] = high
        d_ref[CH : 2 * CH, COLS * part : COLS * (part + 1)] = low
    arrive(fetch([(d_ref, d_hbm)], sems))


def pushes(value, drive, push):
    push[...] = jnp.dot(jnp.concatenate([value, value], axis=1), drive[...], preferred_element_type=f32)


def project_kernel(*refs):
    blocks, weights, drive_hbm, t = refs[:8], refs[8:12], refs[12], refs[13]
    mixed, payload_hbm, payload, ordered, drive, push, sems = refs[14:]
    z, x, y, c = where_am_i()
    (drive_copy,) = fetch([(drive_hbm, drive)], sems)
    squares = blocks[0][ROWS:, 0:ROWS].astype(f32)
    for block in blocks[1:]:
        squares += block[ROWS:, 0:ROWS].astype(f32)
    squares = jnp.sum(jnp.transpose(squares), axis=1, keepdims=True) * 0.125
    inverse = lax.rsqrt(squares / WIDTH + epsilon)
    for k in range(RING):
        for u in range(RING):
            from_z, from_x = jnp.where(c == 0, ring(z, k), u), jnp.where(c == 0, u, ring(x, k))
            ordered[from_z, from_x] = weights[k][u]
    total = jnp.zeros((ROWS, 2 * CH), f32)
    for k in range(RING):
        at = ring(y, k)
        left = jnp.concatenate([blocks[k][0:ROWS], blocks[k + 4][0:ROWS]], axis=1)
        right = [ordered[at, pl.ds(2 * core, 2)].reshape(SLICE, 2 * CH) for core in (c, 1 - c)]
        total += jnp.dot(left, jnp.concatenate(right, axis=0), preferred_element_type=f32)
    value = (total * inverse).astype(bf16)
    mixed[...] = value
    drive_copy.wait()
    pushes(value[:, 0:CH], drive, push)
    sums = [(jnp.zeros((8, 128), f32), jnp.zeros((8, 128), f32)) for _ in range(4)]
    for k in range(ROWS // 8):
        for j in range(4):
            at_r, at_i = slice(128 * j, 128 * (j + 1)), slice(COLS + 128 * j, COLS + 128 * (j + 1))
            by_r, by_i = t[7:8, at_r], t[15:16, at_r]
            real, imag = push[8 * k : 8 * k + 8, at_r], push[8 * k : 8 * k + 8, at_i]
            old_r, old_i = sums[j]
            sums[j] = (real + (old_r * by_r - old_i * by_i), imag + (old_r * by_i + old_i * by_r))
    for j, (real, imag) in enumerate(sums):
        cols = slice(128 * j, 128 * (j + 1))
        by_r, by_i = t[16:24, cols], t[24:32, cols]
        payload[j : j + 1] = jnp.sum(real * by_r - imag * by_i, axis=0, keepdims=True)
        payload[4 + j : 5 + j] = jnp.sum(real * by_i + imag * by_r, axis=0, keepdims=True)
    payload[8:24] = value[ROWS - HALO :, CH : 2 * CH].astype(f32)
    arrive(fetch([(payload, payload_hbm.at[peer]) for peer in range(16)], sems))


def local_kernel(
    mixed, drive, t, outr, outi, pw, skip, gain, keep, r, push, outr_v, outi_v, pw_v, skip_v, gain_v, sems
):
    z, x, y, c = where_am_i()
    s = z * RING + x
    coming = fetch(
        [
            (heads_of(outr), outr_v),
            (heads_of(outi), outi_v),
            (pw.at[pl.ds((y * 2 + c) * 2, 2)], pw_v),
            (skip, skip_v),
            (gain, gain_v),
        ],
        sems,
    )
    row = iota((8, COLS), 0)
    by_r, by_i = t[7:8], t[15:16]
    for _ in range(5):
        by_r, by_i = by_r * by_r - by_i * by_i, 2.0 * by_r * by_i
    gap = s - 1 - iota((16, COLS), 0)
    real, imag = jnp.where(gap >= 0, 1.0, 0.0), jnp.zeros((16, COLS), f32)
    for bit in range(4):
        on = (jnp.maximum(gap, 0) >> bit) % 2 == 1
        real, imag = (
            jnp.where(on, real * by_r - imag * by_i, real),
            jnp.where(on, real * by_i + imag * by_r, imag),
        )
        by_r, by_i = by_r * by_r - by_i * by_i, 2.0 * by_r * by_i
    keep[ROWS : ROWS + 16, 0:COLS], keep[ROWS : ROWS + 16, COLS:] = real, imag

    pushes(mixed[:, 0:CH], drive, push)
    for j in range(4):
        at_r, at_i = slice(128 * j, 128 * (j + 1)), slice(COLS + 128 * j, COLS + 128 * (j + 1))
        levels = []
        for by in (1, 2, 4):
            far = row[:, 0:128] >= by
            levels.append((by, jnp.where(far, t[by - 1 : by, at_r], 0.0), jnp.where(far, t[by + 7 : by + 8, at_r], 0.0)))
        for k in range(ROWS // 8):
            rows = slice(8 * k, 8 * k + 8)
            real, imag = push[rows, at_r], push[rows, at_i]
            for by, mul_r, mul_i in levels:
                old_r, old_i = pltpu.roll(real, by, 0), pltpu.roll(imag, by, 0)
                real, imag = real + mul_r * old_r - mul_i * old_i, imag + mul_r * old_i + mul_i * old_r
            keep[rows, at_r] = real
            keep[rows, at_i] = imag

    arrive(coming)
    spread = spread_of(CH)
    for part, (value, sign) in enumerate(((outr_v, 1.0), (outi_v, -1.0))):
        high, low = split(sign * across(value, spread))
        r[0:CH, COLS * part : COLS * (part + 1)] = high
        r[CH : 2 * CH, COLS * part : COLS * (part + 1)] = low
    pick = (iota((64, CH), 0) == iota((64, CH), 1) % 64).astype(bf16)
    wide = jnp.dot(pw_v[...].reshape(CH, 64), pick, preferred_element_type=f32)
    wide = jnp.where(iota((CH, CH), 0) // 64 == iota((CH, CH), 1) // 64, wide, 0.0).astype(bf16)
    r[0:CH, 2 * COLS :] = wide
    r[CH : 2 * CH, 2 * COLS :] = wide
    me = y * 2 + c
    keep[ROWS + 16 : ROWS + 24, 0:128] = jnp.broadcast_to(skip_v[pl.ds(me, 1)], (8, 128))
    keep[ROWS + 16 : ROWS + 24, 128:256] = jnp.broadcast_to(gain_v[pl.ds(me, 1)], (8, 128))


def mix_kernel(x_ref, ends, t, r, mixed, outs, high, low):
    z, x, y, c = where_am_i()
    s = z * RING + x
    me = y * 2 + c
    carries = []
    for j in range(4):
        cols = slice(128 * j, 128 * (j + 1))
        real, imag = ends[:, j, :], ends[:, 4 + j, :]
        at = slice(COLS + 128 * j, COLS + 128 * (j + 1))
        mul_r, mul_i = x_ref[ROWS : ROWS + 16, cols], x_ref[ROWS : ROWS + 16, at]
        carries.append(
            [
                jnp.sum(mul_r * real - mul_i * imag, axis=0, keepdims=True),
                jnp.sum(mul_r * imag + mul_i * real, axis=0, keepdims=True),
            ]
        )
    for k in range(ROWS // 16):
        for j in range(4):
            at_r, at_i = slice(128 * j, 128 * (j + 1)), slice(COLS + 128 * j, COLS + 128 * (j + 1))
            base_r, base_i = t[0:8, at_r], t[8:16, at_r]
            both_r, both_i = [], []
            for h in range(2):
                rows = slice(16 * k + 8 * h, 16 * k + 8 * h + 8)
                old_r, old_i = carries[j]
                real = x_ref[rows, at_r] + (base_r * old_r - base_i * old_i)
                imag = x_ref[rows, at_i] + (base_r * old_i + base_i * old_r)
                carries[j] = [real[7:8], imag[7:8]]
                both_r.append(real)
                both_i.append(imag)
            rows = slice(16 * k, 16 * k + 16)
            for at, both in ((at_r, both_r), (at_i, both_i)):
                high[rows, at], low[rows, at] = split(jnp.concatenate(both, axis=0))
    wide = nt(high[...], r[:, 0 : 2 * COLS])
    total = wide[:, 0:CH] + (wide[:, CH : 2 * CH] + nt(low[...], r[0:CH, 0 : 2 * COLS]))
    total = total + x_ref[ROWS + 16 : ROWS + 17, 0:128] * mixed[:, 0:CH].astype(f32)
    state_out = jax.nn.gelu(total)

    own = mixed[:, CH : 2 * CH].astype(f32)
    halo = jnp.where(s > 0, ends[jnp.maximum(s - 1, 0), 8:24, :], 0.0)
    ext = jnp.concatenate([halo, own], axis=0)
    sums = []
    for k in range(4):
        ext = ext + pltpu.roll(ext, 1 << k, 0)
        sums.append(ext[HALO:])
    lane = iota((ROWS, CH), 1)
    odd = me % 2 == 1
    near = jnp.where(odd, sums[2], sums[0])
    far = jnp.where(odd, sums[3], sums[1])
    window = jnp.where(odd, jnp.where(lane < 64, 8, 16), jnp.where(lane < 64, 2, 4))
    count = jnp.minimum(s * ROWS + 1 + iota((ROWS, CH), 0), window).astype(f32)
    pooled = jnp.where(lane < 64, near, far) / count - own
    pair = jnp.concatenate(split(pooled), axis=1)
    pool_out = jnp.dot(pair, r[:, 2 * COLS :], preferred_element_type=f32) * x_ref[ROWS + 16 : ROWS + 17, 128:256]
    outs[:, 0:CH] = jnp.where(lane < 64, state_out, pltpu.roll(pool_out, 64, 1)).astype(bf16)
    outs[:, CH : 2 * CH] = jnp.where(lane < 64, pltpu.roll(state_out, 64, 1), pool_out).astype(bf16)


def hold_out_kernel(m0, m1, m3, held, sems):
    z, x, c = (lax.axis_index(a) for a in ("z", "x", "c"))

    def copies(core):
        blocks = ((0, m0), (1, m1), (3, m3))
        places = [held.at[ring(x, k)] if core == 0 else held.at[:, ring(z, k)] for k, _ in blocks]
        return [pltpu.make_async_copy(m, place, sems.at[k]) for (k, m), place in zip(blocks, places)]

    for core in range(2):

        @pl.when(c == core)
        def _(core=core):
            started = copies(core)
            for copy in started:
                copy.start()
            arrive(started)


def block_products(blocks, from_c, held, far, rows):
    z, x, y, c = where_am_i()
    total = None
    for k, block in enumerate(blocks):
        from_z = ring(y, k)
        right = []
        for h in range(2):
            from_x = from_c * 2 + h
            last = jnp.where(c == 0, from_x == ring(x, 2), from_z == ring(z, 2))
            weight = jnp.where(last, far[jnp.where(c == 0, from_z, from_x)], held[from_x, from_z])
            right.append(weight.reshape(CH, SLICE))
        part = jnp.dot(block[rows], jnp.concatenate(right, axis=0), preferred_element_type=f32)
        total = part if total is None else total + part
    return total


def direct_kernel(b0, b1, b2, b3, held, far, total):
    total[...] = block_products((b0, b1, b2, b3), lax.axis_index("c"), held, far, slice(0, ROWS))


def final_kernel(b0, b1, b2, b3, held, far, total, out_hbm, out, sems):
    copies = []
    for h in range(2):
        rows = slice(h * ROWS // 2, (h + 1) * ROWS // 2)
        value = total[rows] + block_products((b0, b1, b2, b3), 1 - lax.axis_index("c"), held, far, rows)
        out[rows] = value.astype(bf16)
        copies.append(pltpu.make_async_copy(out.at[rows], out_hbm.at[rows], sems.at[h]))
        copies[h].start()
    arrive(copies)


def shift(value, axis, by):
    return lax.ppermute(value, axis, [(i, (i + by) % RING) for i in range(RING)])


def around(value, axis):
    return [value, *(shift(value, axis, k) for k in range(1, RING))]


def along(value, which):
    parts = [value]
    for by in range(1, RING):
        pairs = []
        for z in range(RING):
            for x in range(RING):
                for c in range(2):
                    to_z, to_x = (z, (x + by) % RING) if which == c else ((z + by) % RING, x)
                    pairs.append(((z * RING + x) * 2 + c, (to_z * RING + to_x) * 2 + c))
        parts.append(lax.ppermute(value, ("z", "x", "c"), pairs))
    return parts


def partner(value):
    return lax.ppermute(value, "c", [(0, 1), (1, 0)])


def body(
    tokens,
    norm_gain,
    state_in_weight,
    pool_in_weight,
    rate_real,
    rate_imag,
    log_step,
    input_real,
    input_imag,
    output_real,
    output_imag,
    skip_gain,
    pool_weight,
    pool_gain,
    state_out_weight,
    pool_out_weight,
):
    rows_in, rows_out, scaled = call(
        pack_kernel,
        [((192, 2 * CH), bf16), ((2, 64, SLICE), bf16), ((ROWS + 16, SLICE), bf16)],
        state_in_weight,
        pool_in_weight,
        state_out_weight,
        pool_out_weight,
        tokens,
        norm_gain.reshape(24, 128),
        hbm=(0, 1, 2, 3, 4, 5),
        scratch=[pltpu.VMEM((ROWS, SLICE), bf16), pltpu.VMEM((24, 128), f32), pltpu.SemaphoreType.DMA((6,))],
    )
    joined_in = join_ring(along(rows_in, 0), 0, "join_in")
    in_weights = along(joined_in, 1)
    joined_out = join_ring(along(rows_out, 1), 1, "join_out")
    out_weights = along(joined_out, 0)
    over_y = around(scaled, "y")
    blocks = over_y + [partner(part) for part in over_y]

    small = [pltpu.VMEM((GROUPS, 64), f32)] * 2 + [pltpu.VMEM((GROUPS, 16, 64), f32)] * 2
    drive, table = call(
        tables_kernel,
        [((2 * CH, 2 * COLS), bf16, "hbm"), ((32, COLS), f32)],
        rate_real,
        rate_imag,
        log_step.reshape(1, 64),
        input_real.swapaxes(1, 2),
        input_imag.swapaxes(1, 2),
        hbm=(0, 1, 2, 3, 4),
        scratch=[
            *small,
            pltpu.VMEM((2 * CH, 2 * COLS), bf16),
            pltpu.VMEM((1, 64), f32),
            pltpu.SemaphoreType.DMA((5,)),
        ],
    )
    mixed, payload = call(
        project_kernel,
        [((ROWS, 2 * CH), bf16), ((16, 24, 128), f32, "hbm")],
        *blocks,
        *in_weights,
        drive,
        table,
        hbm=(12,),
        scratch=[
            pltpu.VMEM((24, 128), f32),
            pltpu.VMEM((RING, RING, 192, 2 * CH), bf16),
            pltpu.VMEM((2 * CH, 2 * COLS), bf16),
            pltpu.VMEM((ROWS, 2 * COLS), f32),
            pltpu.SemaphoreType.DMA((16,)),
        ],
    )
    ends = lax.all_to_all(payload, SP, 0, 0, tiled=True)
    local, read = call(
        local_kernel,
        [((ROWS + 24, 2 * COLS), f32), ((2 * CH, 2 * COLS + CH), bf16)],
        mixed,
        drive,
        table,
        output_real,
        output_imag,
        pool_weight,
        skip_gain.reshape(8, 128),
        pool_gain.reshape(8, 128),
        hbm=(3, 4, 5, 6, 7),
        scratch=[
            pltpu.VMEM((ROWS, 2 * COLS), f32),
            *small[2:],
            pltpu.VMEM((2, 64, 64), bf16),
            pltpu.VMEM((8, 128), f32),
            pltpu.VMEM((8, 128), f32),
            pltpu.SemaphoreType.DMA((6,)),
        ],
    )
    outs = call(
        mix_kernel,
        [((ROWS, 2 * CH), bf16)],
        local,
        ends,
        table,
        read,
        mixed,
        scratch=[pltpu.VMEM((ROWS, 2 * COLS), bf16), pltpu.VMEM((ROWS, 2 * COLS), bf16)],
    )
    over_y = around(outs, "y")
    over_c = [partner(part) for part in over_y]
    own, one, far, three = out_weights
    held = call(
        hold_out_kernel,
        [((RING, RING, 2, 64, SLICE), bf16)],
        own,
        one,
        three,
        anywhere=(0, 1, 2),
        scratch=[pltpu.SemaphoreType.DMA((4,))],
    )
    total = call(direct_kernel, [((ROWS, SLICE), f32)], *over_y, held, far)
    return call(
        final_kernel,
        [((ROWS, SLICE), bf16, "hbm")],
        *over_c,
        held,
        far,
        total,
        scratch=[pltpu.VMEM((ROWS, SLICE), bf16), pltpu.SemaphoreType.DMA((2,))],
    )


def solution(mesh):
    finer = Mesh(mesh.devices.reshape(4, 4, 4, 2), ("z", "x", "y", "c"))
    split_specs = P(SP, TP)
    in_specs = (
        split_specs, P(), split_specs, split_specs, P(), P(), P(), P(), P(), P(), P(), P(), P(), P(), split_specs, split_specs,
    )

    return jax.shard_map(body, mesh=finer, in_specs=in_specs, out_specs=split_specs, check_vma=False)
```

```python
import jax
import jax.numpy as jnp
from jax import lax
from jax.experimental import pallas as pl
from jax.experimental.pallas import tpu as pltpu
from jax.sharding import Mesh
from jax.sharding import PartitionSpec as P

SP = ("z", "x")
TP = ("y", "c")
RING = 4
ROWS = 256
WIDTH = 3072
SLICE = 384
LENGTH = 4096
CH = 128
GROUPS = 8
COLS = 512
HALO = 16
epsilon = 1e-06

bf16, f32 = jnp.bfloat16, jnp.float32


def call(body, outs, *args, scratch=(), hbm=(), anywhere=(), limit=8, name=None):
    vmem_spec, hbm_spec = (pl.BlockSpec(memory_space=space) for space in (pltpu.VMEM, pltpu.HBM))
    shapes, out_specs = [], []
    for shape, dtype, *where in outs:
        kind = {"": pltpu.VMEM, "hbm": pltpu.HBM, "last": jax.ShapeDtypeStruct}[where[0] if where else ""]
        shapes.append(kind(shape, dtype))
        out_specs.append(hbm_spec if where == ["hbm"] else vmem_spec)
    held, in_specs = [], []
    for k, arg in enumerate(args):
        if k in anywhere:
            held.append(arg)
            in_specs.append(pl.BlockSpec(memory_space=pl.ANY))
        else:
            held.append(pltpu.with_memory_space_constraint(arg, pltpu.HBM if k in hbm else pltpu.VMEM))
            in_specs.append(hbm_spec if k in hbm else vmem_spec)
    name = name or body.__name__.removesuffix("_kernel")
    single = len(outs) == 1
    return pl.pallas_call(
        body,
        out_shape=shapes[0] if single else shapes,
        in_specs=in_specs,
        out_specs=out_specs[0] if single else out_specs,
        scratch_shapes=list(scratch),
        compiler_params=pltpu.CompilerParams(vmem_limit_bytes=limit << 20),
    )(*held)


def fetch(moves, sems):
    copies = [pltpu.make_async_copy(src, dst, sems.at[k]) for k, (src, dst) in enumerate(moves)]
    for copy in copies:
        copy.start()
    return copies


def arrive(copies):
    for copy in copies:
        copy.wait()


def iota(shape, dim):
    return lax.broadcasted_iota(jnp.int32, shape, dim)


def where_am_i():
    z, x, y, c = (lax.axis_index(a) for a in ("z", "x", "y", "c"))
    return z, x, y, c


def ring(index, back):
    return lax.rem(index + RING - back, RING)


def nt(a, b):
    return lax.dot_general(a, b, (((1,), (1,)), ((), ())), preferred_element_type=f32)


def split(value):
    high = value.astype(bf16)
    return high, (value - high.astype(f32)).astype(bf16)


def pack_kernel(ws, wp, os, op, tokens, gain, rows_in, rows_out, scaled, tokens_v, gain_v, sems):
    copies = fetch(
        [
            (gain, gain_v),
            (tokens, tokens_v),
            (ws, rows_in.at[:, pl.ds(0, CH)]),
            (wp, rows_in.at[:, pl.ds(CH, CH)]),
            (os, rows_out.at[0]),
            (op, rows_out.at[1]),
        ],
        sems,
    )
    t = lax.axis_index("y") * 2 + lax.axis_index("c")
    arrive(copies[:2])
    squares = jnp.zeros((16, ROWS), f32)
    ones = jnp.ones((16, 128), bf16)
    for j in range(3):
        cols = slice(128 * j, 128 * (j + 1))
        value = tokens_v[:, cols].astype(f32)
        scaled[0:ROWS, cols] = (value * gain_v[pl.ds(3 * t + j, 1)]).astype(bf16)
        for part in split(value * value):
            squares += nt(ones, part)
    high = squares.astype(bf16).astype(f32)
    scaled[ROWS:, 0:ROWS] = jnp.where(iota((16, ROWS), 0) < 8, high, squares - high).astype(bf16)
    scaled[ROWS:, ROWS:] = jnp.zeros((16, SLICE - ROWS), bf16)
    arrive(copies[2:])


def axis_index_of(which):
    x, z = lax.axis_index("x"), lax.axis_index("z")
    return jnp.where(lax.axis_index("c") == which, x, z)


def join_ring(parts, which, name):
    def body(m0, m1, m2, m3, joined):
        index = axis_index_of(which)
        for k, m in enumerate((m0, m1, m2, m3)):
            joined[ring(index, k)] = m[...]

    return call(body, [((RING, *parts[0].shape), parts[0].dtype)], *parts, name=name)


def spread_of(rows):
    return (iota((rows, COLS), 0) % 64 == iota((rows, COLS), 1) % 64).astype(bf16)


def across(value, spread):
    pair = jnp.concatenate(split(value[...].reshape(CH, 64)), axis=1)
    wide = jnp.dot(pair, spread, preferred_element_type=f32)
    return jnp.where(iota((CH, COLS), 0) // 16 == iota((CH, COLS), 1) // 64, wide, 0.0)


def heads_of(array):
    t = lax.axis_index("y") * 2 + lax.axis_index("c")
    return array.at[pl.ds(pl.multiple_of(t * GROUPS, GROUPS), GROUPS)]


def tables_kernel(rr, ri, ls_hbm, inr, ini, d_hbm, t_ref, rr_v, ri_v, inr_v, ini_v, d_ref, ls, sems):
    g0 = (lax.axis_index("y") * 2 + lax.axis_index("c")) * GROUPS
    arrive(fetch([(heads_of(rr), rr_v), (heads_of(ri), ri_v), (heads_of(inr), inr_v), (heads_of(ini), ini_v), (ls_hbm, ls)], sems))

    spread = spread_of(CH)
    own_row = iota((GROUPS, COLS), 1) // 64 == iota((GROUPS, COLS), 0)

    def flat(value):
        high, low = split(value)
        rest = (value - high.astype(f32)) - low.astype(f32)
        wide = jnp.dot(jnp.concatenate([high, low], axis=1), spread, preferred_element_type=f32)
        wide = wide + jnp.dot(rest.astype(bf16), spread[0:64], preferred_element_type=f32)
        return jnp.sum(jnp.where(own_row, wide, 0.0), axis=0, keepdims=True)

    logs = jnp.broadcast_to(ls[...], (GROUPS, 64))
    mine = iota((GROUPS, 64), 1) == iota((GROUPS, 64), 0) + g0
    step = jnp.exp(jnp.sum(jnp.where(mine, logs, 0.0), axis=1, keepdims=True)) / LENGTH
    rate_r, rate_i = flat(rr_v[...]), flat(ri_v[...])
    step = flat(jnp.broadcast_to(step, (GROUPS, 64)))
    exponent, angle = rate_r * step, rate_i * step
    row = iota((8, COLS), 0)
    for first, count in ((0, row + 1), (16, 7 - row)):
        count = count.astype(f32)
        size = jnp.exp(exponent * count)
        t_ref[first : first + 8] = size * jnp.cos(angle * count)
        t_ref[first + 8 : first + 16] = size * jnp.sin(angle * count)
    decay_i = t_ref[8:9]
    grown = exponent * (1.0 + exponent * (0.5 + exponent * (1.0 / 6.0 + exponent * (1.0 / 24.0))))
    half = jnp.sin(0.5 * angle)
    less_one = grown * jnp.cos(angle) - 2.0 * half * half
    below = rate_r * rate_r + rate_i * rate_i
    factor_r = (less_one * rate_r + decay_i * rate_i) / below
    factor_i = (decay_i * rate_r - less_one * rate_i) / below

    in_r, in_i = across(inr_v, spread), across(ini_v, spread)
    for part, value in ((0, factor_r * in_r - factor_i * in_i), (1, factor_r * in_i + factor_i * in_r)):
        high, low = split(value)
        d_ref[0:CH, COLS * part : COLS * (part + 1)] = high
        d_ref[CH : 2 * CH, COLS * part : COLS * (part + 1)] = low
    arrive(fetch([(d_ref, d_hbm)], sems))


def pushes(value, drive, push):
    push[...] = jnp.dot(jnp.concatenate([value, value], axis=1), drive[...], preferred_element_type=f32)


def project_kernel(*refs):
    blocks, weights, drive_hbm, t = refs[:8], refs[8:12], refs[12], refs[13]
    mixed, payload_hbm, payload, ordered, total, drive, push, sems = refs[14:]
    z, x, y, c = where_am_i()
    (drive_copy,) = fetch([(drive_hbm, drive)], sems)
    squares = blocks[0][ROWS:, 0:ROWS].astype(f32)
    for block in blocks[1:]:
        squares += block[ROWS:, 0:ROWS].astype(f32)
    squares = jnp.sum(jnp.transpose(squares), axis=1, keepdims=True) * 0.125
    inverse = lax.rsqrt(squares / WIDTH + epsilon)

    def left(k):
        return jnp.concatenate([blocks[k][0:ROWS], blocks[k + 4][0:ROWS]], axis=1)

    gap = lax.rem(y - z + RING, RING)
    for variant in range(RING):

        @pl.when((c == 0) & (gap == variant))
        def _(variant=variant):
            value = jnp.zeros((ROWS, 2 * CH), f32)
            for j in range(RING):
                right = weights[j][...].reshape(2 * SLICE, 2 * CH)
                value += jnp.dot(left((variant + j) % RING), right, preferred_element_type=f32)
            total[...] = value

    @pl.when(c == 1)
    def _():
        for k in range(RING):
            for u in range(RING):
                ordered[u, ring(x, k)] = weights[k][u]
        value = jnp.zeros((ROWS, 2 * CH), f32)
        for k in range(RING):
            right = [ordered[ring(y, k), 2 * core : 2 * core + 2].reshape(SLICE, 2 * CH) for core in (1, 0)]
            value += jnp.dot(left(k), jnp.concatenate(right, axis=0), preferred_element_type=f32)
        total[...] = value

    value = (total[...] * inverse).astype(bf16)
    mixed[...] = value
    drive_copy.wait()
    pushes(value[:, 0:CH], drive, push)
    sums = [(jnp.zeros((8, 128), f32), jnp.zeros((8, 128), f32)) for _ in range(4)]
    for k in range(ROWS // 8):
        for j in range(4):
            at_r, at_i = slice(128 * j, 128 * (j + 1)), slice(COLS + 128 * j, COLS + 128 * (j + 1))
            by_r, by_i = t[7:8, at_r], t[15:16, at_r]
            real, imag = push[8 * k : 8 * k + 8, at_r], push[8 * k : 8 * k + 8, at_i]
            old_r, old_i = sums[j]
            sums[j] = (real + (old_r * by_r - old_i * by_i), imag + (old_r * by_i + old_i * by_r))
    for j, (real, imag) in enumerate(sums):
        cols = slice(128 * j, 128 * (j + 1))
        by_r, by_i = t[16:24, cols], t[24:32, cols]
        payload[j : j + 1] = jnp.sum(real * by_r - imag * by_i, axis=0, keepdims=True)
        payload[4 + j : 5 + j] = jnp.sum(real * by_i + imag * by_r, axis=0, keepdims=True)
    payload[8:24] = value[ROWS - HALO :, CH : 2 * CH].astype(f32)
    arrive(fetch([(payload, payload_hbm.at[peer]) for peer in range(16)], sems))


def local_kernel(
    mixed, drive, t, outr, outi, pw, skip, gain, keep, r, push, outr_v, outi_v, pw_v, skip_v, gain_v, sems
):
    z, x, y, c = where_am_i()
    s = z * RING + x
    coming = fetch(
        [
            (heads_of(outr), outr_v),
            (heads_of(outi), outi_v),
            (pw.at[pl.ds((y * 2 + c) * 2, 2)], pw_v),
            (skip, skip_v),
            (gain, gain_v),
        ],
        sems,
    )
    row = iota((8, COLS), 0)
    by_r, by_i = t[7:8], t[15:16]
    for _ in range(5):
        by_r, by_i = by_r * by_r - by_i * by_i, 2.0 * by_r * by_i
    gap = s - 1 - iota((16, COLS), 0)
    real, imag = jnp.where(gap >= 0, 1.0, 0.0), jnp.zeros((16, COLS), f32)
    for bit in range(4):
        on = (jnp.maximum(gap, 0) >> bit) % 2 == 1
        real, imag = (
            jnp.where(on, real * by_r - imag * by_i, real),
            jnp.where(on, real * by_i + imag * by_r, imag),
        )
        by_r, by_i = by_r * by_r - by_i * by_i, 2.0 * by_r * by_i
    keep[ROWS : ROWS + 16, 0:COLS], keep[ROWS : ROWS + 16, COLS:] = real, imag

    pushes(mixed[:, 0:CH], drive, push)
    for j in range(4):
        at_r, at_i = slice(128 * j, 128 * (j + 1)), slice(COLS + 128 * j, COLS + 128 * (j + 1))
        levels = []
        for by in (1, 2, 4):
            far = row[:, 0:128] >= by
            levels.append((by, jnp.where(far, t[by - 1 : by, at_r], 0.0), jnp.where(far, t[by + 7 : by + 8, at_r], 0.0)))
        for k in range(ROWS // 8):
            rows = slice(8 * k, 8 * k + 8)
            real, imag = push[rows, at_r], push[rows, at_i]
            for by, mul_r, mul_i in levels:
                old_r, old_i = pltpu.roll(real, by, 0), pltpu.roll(imag, by, 0)
                real, imag = real + mul_r * old_r - mul_i * old_i, imag + mul_r * old_i + mul_i * old_r
            keep[rows, at_r] = real
            keep[rows, at_i] = imag

    arrive(coming)
    spread = spread_of(CH)
    for part, (value, sign) in enumerate(((outr_v, 1.0), (outi_v, -1.0))):
        high, low = split(sign * across(value, spread))
        r[0:CH, COLS * part : COLS * (part + 1)] = high
        r[CH : 2 * CH, COLS * part : COLS * (part + 1)] = low
    pick = (iota((64, CH), 0) == iota((64, CH), 1) % 64).astype(bf16)
    wide = jnp.dot(pw_v[...].reshape(CH, 64), pick, preferred_element_type=f32)
    wide = jnp.where(iota((CH, CH), 0) // 64 == iota((CH, CH), 1) // 64, wide, 0.0).astype(bf16)
    r[0:CH, 2 * COLS :] = wide
    r[CH : 2 * CH, 2 * COLS :] = wide
    me = y * 2 + c
    keep[ROWS + 16 : ROWS + 24, 0:128] = jnp.broadcast_to(skip_v[pl.ds(me, 1)], (8, 128))
    keep[ROWS + 16 : ROWS + 24, 128:256] = jnp.broadcast_to(gain_v[pl.ds(me, 1)], (8, 128))


def mix_kernel(x_ref, ends, t, r, mixed, outs, high, low):
    z, x, y, c = where_am_i()
    s = z * RING + x
    me = y * 2 + c
    carries = []
    for j in range(4):
        cols = slice(128 * j, 128 * (j + 1))
        real, imag = ends[:, j, :], ends[:, 4 + j, :]
        at = slice(COLS + 128 * j, COLS + 128 * (j + 1))
        mul_r, mul_i = x_ref[ROWS : ROWS + 16, cols], x_ref[ROWS : ROWS + 16, at]
        carries.append(
            [
                jnp.sum(mul_r * real - mul_i * imag, axis=0, keepdims=True),
                jnp.sum(mul_r * imag + mul_i * real, axis=0, keepdims=True),
            ]
        )
    for k in range(ROWS // 16):
        for j in range(4):
            at_r, at_i = slice(128 * j, 128 * (j + 1)), slice(COLS + 128 * j, COLS + 128 * (j + 1))
            base_r, base_i = t[0:8, at_r], t[8:16, at_r]
            both_r, both_i = [], []
            for h in range(2):
                rows = slice(16 * k + 8 * h, 16 * k + 8 * h + 8)
                old_r, old_i = carries[j]
                real = x_ref[rows, at_r] + (base_r * old_r - base_i * old_i)
                imag = x_ref[rows, at_i] + (base_r * old_i + base_i * old_r)
                carries[j] = [real[7:8], imag[7:8]]
                both_r.append(real)
                both_i.append(imag)
            rows = slice(16 * k, 16 * k + 16)
            for at, both in ((at_r, both_r), (at_i, both_i)):
                high[rows, at], low[rows, at] = split(jnp.concatenate(both, axis=0))
    wide = nt(high[...], r[:, 0 : 2 * COLS])
    total = wide[:, 0:CH] + (wide[:, CH : 2 * CH] + nt(low[...], r[0:CH, 0 : 2 * COLS]))
    total = total + x_ref[ROWS + 16 : ROWS + 17, 0:128] * mixed[:, 0:CH].astype(f32)
    state_out = jax.nn.gelu(total)

    own = mixed[:, CH : 2 * CH].astype(f32)
    halo = jnp.where(s > 0, ends[jnp.maximum(s - 1, 0), 8:24, :], 0.0)
    ext = jnp.concatenate([halo, own], axis=0)
    sums = []
    for k in range(4):
        ext = ext + pltpu.roll(ext, 1 << k, 0)
        sums.append(ext[HALO:])
    lane = iota((ROWS, CH), 1)
    odd = me % 2 == 1
    near = jnp.where(odd, sums[2], sums[0])
    far = jnp.where(odd, sums[3], sums[1])
    window = jnp.where(odd, jnp.where(lane < 64, 8, 16), jnp.where(lane < 64, 2, 4))
    count = jnp.minimum(s * ROWS + 1 + iota((ROWS, CH), 0), window).astype(f32)
    pooled = jnp.where(lane < 64, near, far) / count - own
    pair = jnp.concatenate(split(pooled), axis=1)
    pool_out = jnp.dot(pair, r[:, 2 * COLS :], preferred_element_type=f32) * x_ref[ROWS + 16 : ROWS + 17, 128:256]
    outs[:, 0:CH] = jnp.where(lane < 64, state_out, pltpu.roll(pool_out, 64, 1)).astype(bf16)
    outs[:, CH : 2 * CH] = jnp.where(lane < 64, pltpu.roll(state_out, 64, 1), pool_out).astype(bf16)


def hold_out_kernel(m0, m1, m3, held, sems):
    z, x, c = (lax.axis_index(a) for a in ("z", "x", "c"))

    def copies(core):
        blocks = ((0, m0), (1, m1), (3, m3))
        places = [held.at[ring(x, k)] if core == 0 else held.at[:, ring(z, k)] for k, _ in blocks]
        return [pltpu.make_async_copy(m, place, sems.at[k]) for (k, m), place in zip(blocks, places)]

    for core in range(2):

        @pl.when(c == core)
        def _(core=core):
            started = copies(core)
            for copy in started:
                copy.start()
            arrive(started)


def block_products(blocks, from_c, held, far, rows):
    z, x, y, c = where_am_i()
    total = None
    for k, block in enumerate(blocks):
        from_z = ring(y, k)
        right = []
        for h in range(2):
            from_x = from_c * 2 + h
            last = jnp.where(c == 0, from_x == ring(x, 2), from_z == ring(z, 2))
            weight = jnp.where(last, far[jnp.where(c == 0, from_z, from_x)], held[from_x, from_z])
            right.append(weight.reshape(CH, SLICE))
        part = jnp.dot(block[rows], jnp.concatenate(right, axis=0), preferred_element_type=f32)
        total = part if total is None else total + part
    return total


def direct_kernel(b0, b1, b2, b3, held, far, total):
    total[...] = block_products((b0, b1, b2, b3), lax.axis_index("c"), held, far, slice(0, ROWS))


def final_kernel(b0, b1, b2, b3, held, far, total, out_hbm, out, sems):
    copies = []
    for h in range(2):
        rows = slice(h * ROWS // 2, (h + 1) * ROWS // 2)
        value = total[rows] + block_products((b0, b1, b2, b3), 1 - lax.axis_index("c"), held, far, rows)
        out[rows] = value.astype(bf16)
        copies.append(pltpu.make_async_copy(out.at[rows], out_hbm.at[rows], sems.at[h]))
        copies[h].start()
    arrive(copies)


def shift(value, axis, by):
    return lax.ppermute(value, axis, [(i, (i + by) % RING) for i in range(RING)])


def around(value, axis):
    return [value, *(shift(value, axis, k) for k in range(1, RING))]


def along(value, which):
    parts = [value]
    for by in range(1, RING):
        pairs = []
        for z in range(RING):
            for x in range(RING):
                for c in range(2):
                    to_z, to_x = (z, (x + by) % RING) if which == c else ((z + by) % RING, x)
                    pairs.append(((z * RING + x) * 2 + c, (to_z * RING + to_x) * 2 + c))
        parts.append(lax.ppermute(value, ("z", "x", "c"), pairs))
    return parts


def partner(value):
    return lax.ppermute(value, "c", [(0, 1), (1, 0)])


def body(
    tokens,
    norm_gain,
    state_in_weight,
    pool_in_weight,
    rate_real,
    rate_imag,
    log_step,
    input_real,
    input_imag,
    output_real,
    output_imag,
    skip_gain,
    pool_weight,
    pool_gain,
    state_out_weight,
    pool_out_weight,
):
    rows_in, rows_out, scaled = call(
        pack_kernel,
        [((192, 2 * CH), bf16), ((2, 64, SLICE), bf16), ((ROWS + 16, SLICE), bf16)],
        state_in_weight,
        pool_in_weight,
        state_out_weight,
        pool_out_weight,
        tokens,
        norm_gain.reshape(24, 128),
        hbm=(0, 1, 2, 3, 4, 5),
        scratch=[pltpu.VMEM((ROWS, SLICE), bf16), pltpu.VMEM((24, 128), f32), pltpu.SemaphoreType.DMA((6,))],
    )
    joined_in = join_ring(along(rows_in, 0), 0, "join_in")
    in_weights = along(joined_in, 1)
    joined_out = join_ring(along(rows_out, 1), 1, "join_out")
    out_weights = along(joined_out, 0)
    over_y = around(scaled, "y")
    blocks = over_y + [partner(part) for part in over_y]

    small = [pltpu.VMEM((GROUPS, 64), f32)] * 2 + [pltpu.VMEM((GROUPS, 16, 64), f32)] * 2
    drive, table = call(
        tables_kernel,
        [((2 * CH, 2 * COLS), bf16, "hbm"), ((32, COLS), f32)],
        rate_real,
        rate_imag,
        log_step.reshape(1, 64),
        input_real.swapaxes(1, 2),
        input_imag.swapaxes(1, 2),
        hbm=(0, 1, 2, 3, 4),
        scratch=[
            *small,
            pltpu.VMEM((2 * CH, 2 * COLS), bf16),
            pltpu.VMEM((1, 64), f32),
            pltpu.SemaphoreType.DMA((5,)),
        ],
    )
    mixed, payload = call(
        project_kernel,
        [((ROWS, 2 * CH), bf16), ((16, 24, 128), f32, "hbm")],
        *blocks,
        *in_weights,
        drive,
        table,
        hbm=(12,),
        scratch=[
            pltpu.VMEM((24, 128), f32),
            pltpu.VMEM((RING, RING, 192, 2 * CH), bf16),
            pltpu.VMEM((ROWS, 2 * CH), f32),
            pltpu.VMEM((2 * CH, 2 * COLS), bf16),
            pltpu.VMEM((ROWS, 2 * COLS), f32),
            pltpu.SemaphoreType.DMA((16,)),
        ],
    )
    ends = lax.all_to_all(payload, SP, 0, 0, tiled=True)
    local, read = call(
        local_kernel,
        [((ROWS + 24, 2 * COLS), f32), ((2 * CH, 2 * COLS + CH), bf16)],
        mixed,
        drive,
        table,
        output_real,
        output_imag,
        pool_weight,
        skip_gain.reshape(8, 128),
        pool_gain.reshape(8, 128),
        hbm=(3, 4, 5, 6, 7),
        scratch=[
            pltpu.VMEM((ROWS, 2 * COLS), f32),
            *small[2:],
            pltpu.VMEM((2, 64, 64), bf16),
            pltpu.VMEM((8, 128), f32),
            pltpu.VMEM((8, 128), f32),
            pltpu.SemaphoreType.DMA((6,)),
        ],
    )
    outs = call(
        mix_kernel,
        [((ROWS, 2 * CH), bf16)],
        local,
        ends,
        table,
        read,
        mixed,
        scratch=[pltpu.VMEM((ROWS, 2 * COLS), bf16), pltpu.VMEM((ROWS, 2 * COLS), bf16)],
    )
    over_y = around(outs, "y")
    over_c = [partner(part) for part in over_y]
    own, one, far, three = out_weights
    held = call(
        hold_out_kernel,
        [((RING, RING, 2, 64, SLICE), bf16)],
        own,
        one,
        three,
        anywhere=(0, 1, 2),
        scratch=[pltpu.SemaphoreType.DMA((4,))],
    )
    total = call(direct_kernel, [((ROWS, SLICE), f32)], *over_y, held, far)
    return call(
        final_kernel,
        [((ROWS, SLICE), bf16, "hbm")],
        *over_c,
        held,
        far,
        total,
        scratch=[pltpu.VMEM((ROWS, SLICE), bf16), pltpu.SemaphoreType.DMA((2,))],
    )


def solution(mesh):
    finer = Mesh(mesh.devices.reshape(4, 4, 4, 2), ("z", "x", "y", "c"))
    split_specs = P(SP, TP)
    in_specs = (
        split_specs, P(), split_specs, split_specs, P(), P(), P(), P(), P(), P(), P(), P(), P(), P(), split_specs, split_specs,
    )

    return jax.shard_map(body, mesh=finer, in_specs=in_specs, out_specs=split_specs, check_vma=False)
```
